768 devices in a mesh: sp: 384 (over z, y, x), tp: 2 (over core).
Axes of the slice: x: 4, y: 8, z: 12, core: 2. Of those that a mesh axis runs over, the one named last changes fastest.
Arguments:
- queries: bfloat16 [98304, 1024], P('sp', 'tp'), may hold values from -12 to 12
- keys: bfloat16 [98304, 1024], P('sp', 'tp'), may hold values from -6 to 6
- values: bfloat16 [98304, 1024], P('sp', 'tp'), may hold values from -6 to 6
- w_out: bfloat16 [1024, 2048], P(None, 'tp'), may hold values from -0.375 to 0.375
Outputs:
- mixed: bfloat16 [98304, 2048], P('sp', 'tp')
The draws below stay inside these ranges and needn't reach their ends.
All inputs are finite; a program needn't handle non-finite values.
Results may differ from the reference program's by a relative error of at most 0.0056.
Values may be sent and summed in bfloat16 or wider, within the bound.
A program may use at most 64 MiB of HBM per device.

```python
import math
import jax
import jax.numpy as jnp
from jax import lax

HEADS = 8
HEAD_DIM = 128
D = 2048
SIDE_KEY_COUNT = 64
MIDDLE_DILATION = 4
FAR_DILATION = 16
TOKENS = 98304


def draw_queries(key, part):
    shape = (TOKENS, HEADS * HEAD_DIM)
    drawn = jnp.clip(2.0 * jax.random.normal(jax.random.fold_in(key, 1), shape, jnp.float32), -12.0, 12.0)
    return drawn.astype(jnp.bfloat16)


def draw_keys(key, part):
    shape = (TOKENS, HEADS * HEAD_DIM)
    drawn = jnp.clip(jax.random.normal(jax.random.fold_in(key, 2), shape, jnp.float32), -6.0, 6.0)
    return drawn.astype(jnp.bfloat16)


def levels(own_key, shape, split, least, largest):
    def one(dim, blocks):
        draws = jax.random.uniform(jax.random.fold_in(jax.random.fold_in(own_key, 6), dim), (blocks,), jnp.float32, least / len(split), largest / len(split))
        return jnp.repeat(jnp.exp(draws), shape[dim] // blocks).reshape((-1,) + (1,) * (len(shape) - dim - 1))

    loudness = one(*split[0])
    for cut in split[1:]:
        loudness = loudness * one(*cut)
    return loudness


def gaussian(own_key, shape, width, bound, cuts=(), kind=jnp.bfloat16):
    level = levels(own_key, shape, cuts, -0.22, 0.18) if cuts else 1.0
    values = jax.random.normal(own_key, shape, jnp.float32) * width * level
    return jnp.minimum(jnp.maximum(values, -bound), bound).astype(kind)


def setup_inputs(seed: int = 0) -> dict:
    key_of = jax.random.split(jax.random.key(seed), 5)
    queries = draw_queries(jax.random.fold_in(key_of[4], 71), 0)
    keys = draw_keys(jax.random.fold_in(key_of[4], 71), 0)
    values = gaussian(key_of[2], (TOKENS, HEADS * HEAD_DIM), 1.0, 6.0, ((0, 384), (1, 2)))
    w_out = gaussian(key_of[3], (HEADS * HEAD_DIM, D), (HEADS * HEAD_DIM // 4) ** -0.5, 0.375, ((1, 2),))
    return dict(queries=queries, keys=keys, values=values, w_out=w_out)


def block_rows(count):
    return count if count <= 128 else math.gcd(count, 128)


def band_scores(queries, keys, values, dilation_step):
    sequence_length, columns = queries.shape
    heads = columns // HEAD_DIM
    residue_rows = sequence_length // dilation_step
    rows_block = block_rows(residue_rows)
    blocks = residue_rows // rows_block
    span = rows_block + 2 * SIDE_KEY_COUNT
    padding = SIDE_KEY_COUNT * dilation_step
    padded_keys = jnp.pad(keys, ((padding, padding), (0, 0))).reshape(residue_rows + 2 * SIDE_KEY_COUNT, dilation_step, heads, HEAD_DIM)
    padded_values = jnp.pad(values, ((padding, padding), (0, 0))).reshape(residue_rows + 2 * SIDE_KEY_COUNT, dilation_step, heads, HEAD_DIM)
    grouped = queries.reshape(blocks, rows_block, dilation_step, heads, HEAD_DIM)
    query_idx = jnp.arange(rows_block, dtype=jnp.int32)[:, None]
    key_idx = jnp.arange(span, dtype=jnp.int32)[None, :]
    in_band = (key_idx >= query_idx) & (key_idx <= query_idx + 2 * SIDE_KEY_COUNT)
    residues = jnp.arange(dilation_step, dtype=jnp.int32)[:, None, None, None]
    scale = HEAD_DIM ** -0.5

    def one_block(inputs):
        number, query_block = inputs
        first_row = (number * rows_block).astype(jnp.int32)
        key_window = lax.dynamic_slice_in_dim(padded_keys, first_row, span, 0)
        value_window = lax.dynamic_slice_in_dim(padded_values, first_row, span, 0)
        scores = jnp.einsum('qrhe,krhe->rhqk', query_block.astype(jnp.float32), key_window.astype(jnp.float32)) * scale
        key_pos = (first_row + key_idx[None, None] - SIDE_KEY_COUNT) * dilation_step + residues
        allowed = in_band[None, None] & (key_pos >= 0) & (key_pos < sequence_length)
        scores = jnp.where(allowed, scores, -jnp.inf)
        maximum = jnp.max(scores, axis=-1, keepdims=True)
        raised = jnp.exp(scores - maximum)
        denominator = jnp.sum(raised, axis=-1, keepdims=True)
        weights = (raised / denominator).astype(jnp.bfloat16)
        attended = jnp.einsum('rhqk,krhe->qrhe', weights.astype(jnp.float32), value_window.astype(jnp.float32))
        log_den = (maximum + jnp.log(denominator))[..., 0]
        return attended, jnp.transpose(log_den, (2, 0, 1))

    outputs, log_dens = lax.map(one_block, (jnp.arange(blocks, dtype=jnp.int32), grouped))
    return outputs.reshape(sequence_length, heads, HEAD_DIM), log_dens.reshape(sequence_length, heads)


def reference(queries, keys, values, w_out):
    sequence_length, columns = queries.shape
    group_results = [band_scores(queries, keys, values, dilation_step) for dilation_step in (1, MIDDLE_DILATION, FAR_DILATION)]
    stacked_out = jnp.stack([item[0] for item in group_results])
    stacked_den = jnp.stack([item[1] for item in group_results])
    shares = jax.nn.softmax(stacked_den, axis=0)
    attended = jnp.sum(shares[..., None] * stacked_out, axis=0).astype(jnp.bfloat16).reshape(sequence_length, columns)
    return jnp.dot(attended, w_out, preferred_element_type=jnp.float32).astype(jnp.bfloat16)
```

```python
import functools
import math

import jax
import jax.numpy as jnp
from jax import lax
from jax.experimental import pallas as pl
from jax.experimental.pallas import tpu as pltpu
from jax.sharding import PartitionSpec as P

HEAD_DIM = 128
SIDE = 64
ROW = 4
SUB = 4
BLK = 16
MESH = pl.DeviceIdType.MESH
BF, F32 = jnp.bfloat16, jnp.float32
NEG = -1e30
COEF = math.log2(math.e) / math.sqrt(HEAD_DIM)
PEERS = (1, 3, 2)


def attend(q, k, v, bias):
    s = lax.dot_general(q, k, (((1,), (1,)), ((), ())), preferred_element_type=F32)
    t = s * COEF + bias
    m = jnp.max(t, axis=1, keepdims=True)
    p = jnp.exp2(t - m)
    l = jnp.sum(p, axis=1, keepdims=True)
    acc = jnp.dot(p.astype(BF), v, preferred_element_type=F32)
    return m, l, acc


def kernel(
    n, heads, q_hbm, k_hbm, v_hbm, w_hbm, out_ref,
    qn, kn, vn, w, xkv, xq, kvres, qres, sret, sstat, ret, rstat,
    nacc, nm, nl, attm, attp, near_bias, mid_bias, far_bias, lead,
    lsem, xs, xr, ys, yr, ns, nr, rs, rr, ts, tr,
):
    sp, tp = lax.axis_index("sp"), lax.axis_index("tp")
    x = lax.rem(sp, ROW)
    base = sp - x
    up = lax.rem(sp + ROW, n)
    down = lax.rem(sp + n - ROW, n)
    right = lax.rem(sp + 1, n)
    left = lax.rem(sp + n - 1, n)
    rows = qn.shape[0]
    piece = rows // ROW

    loads = [
        pltpu.make_async_copy(k_hbm, kn.at[pl.ds(SIDE, rows)], lsem.at[0]),
        pltpu.make_async_copy(v_hbm, vn.at[pl.ds(SIDE, rows)], lsem.at[1]),
        pltpu.make_async_copy(q_hbm, qn, lsem.at[2]),
        pltpu.make_async_copy(w_hbm, w, lsem.at[3]),
    ]
    for copy in loads:
        copy.start()

    def xpeer(k):
        return lax.rem(x + k, ROW)

    barrier = pltpu.get_barrier_semaphore()
    friends = [(base + xpeer(k), tp) for k in PEERS]
    friends += [(up, tp), (down, tp), (right, tp), (left, tp), (sp, 1 - tp)]
    for friend in friends:
        pl.semaphore_signal(barrier, inc=1, device_id=friend, device_id_type=MESH)

    first = (sp < ROW).astype(jnp.int32)
    last = (sp >= n - ROW).astype(jnp.int32)
    start = (sp == 0).astype(jnp.int32)
    end = (sp == n - 1).astype(jnp.int32)

    def iota(shape, dim):
        return lax.broadcasted_iota(jnp.int32, shape, dim)

    r, t = iota((rows, rows), 0), iota((rows, rows), 1)
    order = (r & 15) * 16 + ((r >> 4) & 3) * 4 + (r >> 6)
    perm = jnp.where(t == order, 1.0, 0.0).astype(BF)
    place = (r & 3) * 64 + ((r >> 2) & 3) * 16 + (r >> 4)
    unperm = jnp.where(t == place, 1.0, 0.0).astype(BF)

    loads[0].wait()
    kp = jnp.dot(perm, kn[SIDE : SIDE + rows], preferred_element_type=F32).astype(BF)
    loads[1].wait()
    vp = jnp.dot(perm, vn[SIDE : SIDE + rows], preferred_element_type=F32).astype(BF)

    def cut(a, c, h):
        a = a[c * piece : (c + 1) * piece, h * HEAD_DIM : (h + 1) * HEAD_DIM]
        return a.reshape(SUB, BLK, HEAD_DIM)

    for h in range(heads):
        for c in range(ROW):
            xkv[c, h, 0] = cut(kp, c, h)
            xkv[c, h, 1] = cut(vp, c, h)
    for h in range(heads):
        kvres[h, :, ROW + x] = xkv[x, h]
    loads[2].wait()
    qp = jnp.dot(perm, qn[...], preferred_element_type=F32).astype(BF)
    for h in range(heads):
        for c in range(ROW):
            xq[c, h] = cut(qp, c, h)
    for h in range(heads):
        qres[h, x] = xq[x, h]

    pl.semaphore_wait(barrier, len(friends))

    def remote(src, dst, ssem, rsem, device):
        return pltpu.make_async_remote_copy(
            src_ref=src, dst_ref=dst, send_sem=ssem, recv_sem=rsem,
            device_id=device, device_id_type=MESH,
        )

    def x_kv(h, k):
        c = xpeer(k)
        return remote(
            xkv.at[c, h], kvres.at[h, :, ROW + x], xs.at[h, k, 0], xr.at[h, k, 0], (base + c, tp)
        )

    def x_q(h, k):
        c = xpeer(k)
        return remote(xq.at[c, h], qres.at[h, x], xs.at[h, k, 1], xr.at[h, k, 1], (base + c, tp))

    def y_kv(h, k, way):
        s = xpeer(ROW - k)
        region = 0 if way == 0 else 2 * ROW
        return remote(
            kvres.at[h, :, ROW + s], kvres.at[h, :, region + s],
            ys.at[h, k, way], yr.at[h, k, way], (up if way == 0 else down, tp),
        )

    def near_copies():
        made = []
        for i, a in enumerate((kn, vn)):
            made.append(remote(
                a.at[pl.ds(rows, SIDE)], a.at[pl.ds(0, SIDE)], ns.at[i, 0], nr.at[i, 0], (right, tp)
            ))
            made.append(remote(
                a.at[pl.ds(SIDE, SIDE)], a.at[pl.ds(SIDE + rows, SIDE)],
                ns.at[i, 1], nr.at[i, 1], (left, tp),
            ))
        return made

    for h in range(heads):
        for k in PEERS:
            x_kv(h, k).start()
        for way in (0, 1):
            y_kv(h, 0, way).start()
    halos = near_copies()
    for h in range(heads):
        for k in PEERS:
            x_q(h, k).start()
        if h == 1:
            for copy in halos:
                copy.start()

    iq, ik = iota((2 * SIDE, 4 * SIDE), 0), iota((2 * SIDE, 4 * SIDE), 1)
    band = (ik >= iq) & (ik <= iq + 2 * SIDE)
    near_bias[0] = jnp.where(band & (ik >= start * SIDE), 0.0, NEG)
    near_bias[1] = jnp.where(band & (ik < 4 * SIDE - end * SIDE), 0.0, NEG)
    iq, ik = iota((SIDE, 3 * SIDE), 0), iota((SIDE, 3 * SIDE), 1)
    low, high = first * SIDE, (3 - last) * SIDE
    inside = (ik >= low) & (ik < high)
    far_bias[...] = jnp.where((ik >= iq) & (ik <= iq + 2 * SIDE) & inside, 0.0, NEG)
    wq = (iq & 15) * 4 + (iq >> 4)
    wk = (ik >> 6) * 64 - SIDE + (ik & 15) * 4 + ((ik >> 4) & 3)
    band = (wk - wq <= SIDE) & (wq - wk <= SIDE)
    mid_bias[0] = jnp.where(band & (ik >= low), 0.0, NEG)
    mid_bias[1] = jnp.where(band, 0.0, NEG)
    mid_bias[2] = mid_bias[1]
    mid_bias[3] = jnp.where(band & (ik < high), 0.0, NEG)
    lead[...] = place[:, :HEAD_DIM]

    for h in range(heads):
        for k in PEERS:
            x_kv(h, k).wait_recv()
            for way in (0, 1):
                y_kv(h, k, way).start()

    def near(h):
        cols = slice(h * HEAD_DIM, (h + 1) * HEAD_DIM)
        for b in range(2):
            span = slice(b * 2 * SIDE, (b + 1) * 2 * SIDE)
            keys = slice(b * 2 * SIDE, b * 2 * SIDE + 4 * SIDE)
            m, l, acc = attend(qn[span, cols], kn[keys, cols], vn[keys, cols], near_bias[b])
            nm[h, span] = m
            nl[h, span] = l
            nacc[h, span] = acc

    def give_back(h, k):
        s = xpeer(k)
        return [
            remote(sret.at[h, s], ret.at[h, x], rs.at[h, k, 0], rr.at[h, k, 0], (base + s, tp)),
            remote(sstat.at[h, s], rstat.at[h, x], rs.at[h, k, 1], rr.at[h, k, 1], (base + s, tp)),
        ]

    def residue(h):
        for k in PEERS:
            x_q(h, k).wait_recv()
        for k in range(ROW):
            for way in (0, 1):
                y_kv(h, k, way).wait_recv()
        far = []
        for d in range(SUB):
            q = qres[h, :, d].reshape(SIDE, HEAD_DIM)
            k = kvres[h, 0, :, d].reshape(3 * SIDE, HEAD_DIM)
            v = kvres[h, 1, :, d].reshape(3 * SIDE, HEAD_DIM)
            far.append(attend(q, k, v, far_bias[...]))
        for s in range(ROW):
            q = qres[h, s].reshape(SIDE, HEAD_DIM)
            k = kvres[h, 0, s + 3 : s + 6].reshape(3 * SIDE, HEAD_DIM)
            v = kvres[h, 1, s + 3 : s + 6].reshape(3 * SIDE, HEAD_DIM)
            m1, l1, acc1 = attend(q, k, v, mid_bias[s])
            part = slice(s * BLK, (s + 1) * BLK)
            m2, l2, acc2 = (
                jnp.concatenate([f[i][part] for f in far], axis=0) for i in range(3)
            )
            m = jnp.maximum(m1, m2)
            a1, a2 = jnp.exp2(m1 - m), jnp.exp2(m2 - m)
            l = a1 * l1 + a2 * l2
            inv = 1.0 / l
            sret[h, s] = ((a1 * inv) * acc1 + (a2 * inv) * acc2).astype(BF)
            lse = jnp.broadcast_to(m + jnp.log2(l), (SIDE, HEAD_DIM))
            flat = jnp.transpose(jnp.concatenate([lse, lse], axis=0))
            sstat[h, s] = flat[:8]
        for k in PEERS:
            for copy in give_back(h, k):
                copy.start()
        ret[h, x] = sret[h, x]
        rstat[h, x] = sstat[h, x]

    def tp_copy(h):
        cols = pl.ds(h * HEAD_DIM, HEAD_DIM)
        return remote(attm.at[:, cols], attp.at[:, cols], ts.at[h], tr.at[h], (sp, 1 - tp))

    def combine(h):
        for k in PEERS:
            for copy in give_back(h, k):
                copy.wait_recv()
        got = ret[h].reshape(rows, HEAD_DIM)
        out = jnp.dot(unperm, got, preferred_element_type=F32)
        lane = iota((rows, HEAD_DIM), 1)
        small = iota((1, HEAD_DIM), 1)
        where = lead[...]
        col = jnp.zeros((rows, HEAD_DIM), F32)
        for pair in range(2):
            row = jnp.where(
                small < piece, rstat[h, 2 * pair, 0:1, :], rstat[h, 2 * pair + 1, 0:1, :]
            )
            col = jnp.where(where == lane + pair * HEAD_DIM, row, col)
        lse = jnp.sum(col, axis=1, keepdims=True)
        m0 = nm[h]
        m = jnp.maximum(m0, lse)
        a0, a1 = jnp.exp2(m0 - m), jnp.exp2(lse - m)
        inv = 1.0 / (a0 * nl[h] + a1)
        att = (a0 * inv) * nacc[h] + (a1 * inv) * out
        attm[:, h * HEAD_DIM : (h + 1) * HEAD_DIM] = att.astype(BF)
        tp_copy(h).start()

    residue(0)
    residue(1)
    for copy in halos:
        copy.wait_recv()
    for h in range(heads):
        near(h)
    residue(2)
    combine(0)
    combine(1)
    residue(3)
    combine(2)
    combine(3)

    loads[3].wait()
    depth = heads * HEAD_DIM
    wm = pl.ds(pl.multiple_of(tp * depth, depth), depth)
    wp = pl.ds(pl.multiple_of((1 - tp) * depth, depth), depth)
    mine = jnp.dot(attm[...], w[wm, :], preferred_element_type=F32)
    for h in range(heads):
        tp_copy(h).wait_recv()
    both = mine + jnp.dot(attp[...], w[wp, :], preferred_element_type=F32)
    out_ref[...] = both.astype(BF)

    for h in range(heads):
        for k in PEERS:
            x_kv(h, k).wait_send()
            x_q(h, k).wait_send()
            for copy in give_back(h, k):
                copy.wait_send()
        for k in range(ROW):
            for way in (0, 1):
                y_kv(h, k, way).wait_send()
        tp_copy(h).wait_send()
    for copy in halos:
        copy.wait_send()


def per_device(n, queries, keys, values, w_out):
    rows, columns = queries.shape
    heads = columns // HEAD_DIM
    width = w_out.shape[1]
    vmem = pltpu.VMEM
    dma = pltpu.SemaphoreType.DMA
    return pl.pallas_call(
        functools.partial(kernel, n, heads),
        out_shape=jax.ShapeDtypeStruct((rows, width), BF),
        in_specs=[pl.BlockSpec(memory_space=pl.ANY)] * 4,
        out_specs=pl.BlockSpec(memory_space=pltpu.VMEM),
        scratch_shapes=[
            vmem((rows, columns), BF),
            vmem((rows + 2 * SIDE, columns), BF),
            vmem((rows + 2 * SIDE, columns), BF),
            vmem(w_out.shape, BF),
            vmem((ROW, heads, 2, SUB, BLK, HEAD_DIM), BF),
            vmem((ROW, heads, SUB, BLK, HEAD_DIM), BF),
            vmem((heads, 2, 3 * ROW, SUB, BLK, HEAD_DIM), BF),
            vmem((heads, ROW, SUB, BLK, HEAD_DIM), BF),
            vmem((heads, ROW, SIDE, HEAD_DIM), BF),
            vmem((heads, ROW, 8, HEAD_DIM), F32),
            vmem((heads, ROW, SIDE, HEAD_DIM), BF),
            vmem((heads, ROW, 8, HEAD_DIM), F32),
            vmem((heads, rows, HEAD_DIM), F32),
            vmem((heads, rows, 1), F32),
            vmem((heads, rows, 1), F32),
            vmem((rows, columns), BF),
            vmem((rows, columns), BF),
            vmem((2, 2 * SIDE, 4 * SIDE), F32),
            vmem((ROW, SIDE, 3 * SIDE), F32),
            vmem((SIDE, 3 * SIDE), F32),
            vmem((rows, HEAD_DIM), jnp.int32),
            dma((4,)),
            dma((heads, ROW, 2)),
            dma((heads, ROW, 2)),
            dma((heads, ROW, 2)),
            dma((heads, ROW, 2)),
            dma((2, 2)),
            dma((2, 2)),
            dma((heads, ROW, 2)),
            dma((heads, ROW, 2)),
            dma((heads,)),
            dma((heads,)),
        ],
        compiler_params=pltpu.CompilerParams(collective_id=0, has_side_effects=True),
        name="fused",
    )(queries, keys, values, w_out)


def solution(mesh):
    return jax.shard_map(
        functools.partial(per_device, mesh.shape["sp"]),
        mesh=mesh,
        in_specs=(P("sp", "tp"), P("sp", "tp"), P("sp", "tp"), P(None, "tp")),
        out_specs=P("sp", "tp"),
        check_vma=False,
    )
```

```python
import functools
import math

import jax
import jax.numpy as jnp
from jax import lax
from jax.experimental import pallas as pl
from jax.experimental.pallas import tpu as pltpu
from jax.sharding import PartitionSpec as P

HEAD_DIM = 128
SIDE = 64
ROW = 4
SUB = 4
BLK = 16
MESH = pl.DeviceIdType.MESH
BF, F32 = jnp.bfloat16, jnp.float32
NEG = -1e30
COEF = math.log2(math.e) / math.sqrt(HEAD_DIM)
PEERS = (1, 3, 2)


def attend(q, k, v, bias):
    s = lax.dot_general(q, k, (((1,), (1,)), ((), ())), preferred_element_type=F32)
    t = s * COEF + bias
    m = jnp.max(t, axis=1, keepdims=True)
    p = jnp.exp2(t - m)
    l = jnp.sum(p, axis=1, keepdims=True)
    acc = jnp.dot(p.astype(BF), v, preferred_element_type=F32)
    return m, l, acc


def kernel(
    n, heads, q_hbm, k_hbm, v_hbm, out_ref,
    qn, kn, vn, xkv, xq, kvres, qres, sret, sstat, ret, rstat,
    nacc, nm, nl, near_bias, mid_bias, far_bias, lead,
    lsem, xs, xr, ys, yr, ns, nr, rs, rr, ts, tr,
):
    sp, tp = lax.axis_index("sp"), lax.axis_index("tp")
    x = lax.rem(sp, ROW)
    base = sp - x
    up = lax.rem(sp + ROW, n)
    down = lax.rem(sp + n - ROW, n)
    right = lax.rem(sp + 1, n)
    left = lax.rem(sp + n - 1, n)
    rows = qn.shape[0]
    piece = rows // ROW

    loads = [
        pltpu.make_async_copy(k_hbm, kn.at[pl.ds(SIDE, rows)], lsem.at[0]),
        pltpu.make_async_copy(v_hbm, vn.at[pl.ds(SIDE, rows)], lsem.at[1]),
        pltpu.make_async_copy(q_hbm, qn, lsem.at[2]),
    ]
    for copy in loads:
        copy.start()

    def xpeer(k):
        return lax.rem(x + k, ROW)

    first = (sp < ROW).astype(jnp.int32)
    last = (sp >= n - ROW).astype(jnp.int32)
    start = (sp == 0).astype(jnp.int32)
    end = (sp == n - 1).astype(jnp.int32)
    to_up, to_down, to_right, to_left = sp < n - ROW, sp >= ROW, sp < n - 1, sp >= 1

    barrier = pltpu.get_barrier_semaphore()

    def greet(friend):
        pl.semaphore_signal(barrier, inc=1, device_id=friend, device_id_type=MESH)

    for k in PEERS:
        greet((base + xpeer(k), tp))
    greet((sp, 1 - tp))
    pl.when(to_up)(lambda: greet((up, tp)))
    pl.when(to_down)(lambda: greet((down, tp)))
    pl.when(to_right)(lambda: greet((right, tp)))
    pl.when(to_left)(lambda: greet((left, tp)))

    def iota(shape, dim):
        return lax.broadcasted_iota(jnp.int32, shape, dim)

    r, t = iota((rows, rows), 0), iota((rows, rows), 1)
    order = (r & 15) * 16 + ((r >> 4) & 3) * 4 + (r >> 6)
    perm = jnp.where(t == order, 1.0, 0.0).astype(BF)
    place = (r & 3) * 64 + ((r >> 2) & 3) * 16 + (r >> 4)
    unperm = jnp.where(t == place, 1.0, 0.0).astype(BF)

    loads[0].wait()
    kp = jnp.dot(perm, kn[SIDE : SIDE + rows], preferred_element_type=F32).astype(BF)
    loads[1].wait()
    vp = jnp.dot(perm, vn[SIDE : SIDE + rows], preferred_element_type=F32).astype(BF)

    def cut(a, c, h):
        a = a[c * piece : (c + 1) * piece, h * HEAD_DIM : (h + 1) * HEAD_DIM]
        return a.reshape(SUB, BLK, HEAD_DIM)

    for h in range(heads):
        for c in range(ROW):
            xkv[c, h, 0] = cut(kp, c, h)
            xkv[c, h, 1] = cut(vp, c, h)

    pl.semaphore_wait(barrier, 2 * ROW - first - last - start - end)

    def remote(src, dst, ssem, rsem, device):
        return pltpu.make_async_remote_copy(
            src_ref=src, dst_ref=dst, send_sem=ssem, recv_sem=rsem,
            device_id=device, device_id_type=MESH,
        )

    def x_kv(h, k):
        c = xpeer(k)
        return remote(
            xkv.at[c, h], kvres.at[h, ROW + x], xs.at[h, k, 0], xr.at[h, k, 0], (base + c, tp)
        )

    def x_q(h, k):
        c = xpeer(k)
        return remote(xq.at[c, h], qres.at[h, x], xs.at[h, k, 1], xr.at[h, k, 1], (base + c, tp))

    def y_kv(h, k, way):
        s = xpeer(ROW - k)
        region = 0 if way == 0 else 2 * ROW
        return remote(
            xkv.at[x, h] if k == 0 else kvres.at[h, ROW + s], kvres.at[h, region + s],
            ys.at[h, k, way], yr.at[h, k, way], (up if way == 0 else down, tp),
        )

    def y_each(act, pairs, sides):
        for way, side in enumerate(sides):
            @pl.when(side)
            def _():
                for h, k in pairs:
                    getattr(y_kv(h, k, way), act)()

    def halo(act, sides):
        for way, side in enumerate(sides):
            @pl.when(side)
            def _():
                for i, a in enumerate((kn, vn)):
                    if way == 0:
                        src, dst, who = pl.ds(rows, SIDE), pl.ds(0, SIDE), right
                    else:
                        src, dst, who = pl.ds(SIDE, SIDE), pl.ds(SIDE + rows, SIDE), left
                    copy = remote(a.at[src], a.at[dst], ns.at[i, way], nr.at[i, way], (who, tp))
                    getattr(copy, act)()

    y_out, y_in = (to_up, to_down), (to_down, to_up)
    halo_out, halo_in = (to_right, to_left), (to_left, to_right)

    for h in range(heads):
        for k in PEERS:
            x_kv(h, k).start()
    y_each("start", [(h, 0) for h in range(heads)], y_out)
    loads[2].wait()
    qp = jnp.dot(perm, qn[...], preferred_element_type=F32).astype(BF)
    for h in range(heads):
        for c in range(ROW):
            xq[c, h] = cut(qp, c, h)
    for h in range(heads):
        for k in PEERS:
            x_q(h, k).start()
    halo("start", halo_out)
    for h in range(heads):
        kvres[h, ROW + x] = xkv[x, h]
        qres[h, x] = xq[x, h]

    blank = jnp.zeros((heads, ROW, 2, SUB, BLK, HEAD_DIM), BF)
    edge = jnp.zeros((SIDE, heads * HEAD_DIM), BF)

    @pl.when(sp < ROW)
    def _():
        kvres[:, :ROW] = blank

    @pl.when(sp >= n - ROW)
    def _():
        kvres[:, 2 * ROW :] = blank

    @pl.when(sp == 0)
    def _():
        kn[:SIDE] = edge
        vn[:SIDE] = edge

    @pl.when(sp == n - 1)
    def _():
        kn[SIDE + rows :] = edge
        vn[SIDE + rows :] = edge

    iq, ik = iota((2 * SIDE, 4 * SIDE), 0), iota((2 * SIDE, 4 * SIDE), 1)
    band = (ik >= iq) & (ik <= iq + 2 * SIDE)
    near_bias[0] = jnp.where(band & (ik >= start * SIDE), 0.0, NEG)
    near_bias[1] = jnp.where(band & (ik < 4 * SIDE - end * SIDE), 0.0, NEG)
    low, high = first * SIDE, (4 - last) * SIDE
    wq = (iq >> 6) * 64 + (iq & 15) * 4 + ((iq >> 4) & 3)
    wk = (ik >> 6) * 64 - SIDE + (ik & 15) * 4 + ((ik >> 4) & 3)
    band = (wk - wq <= SIDE) & (wq - wk <= SIDE)
    mid_bias[0] = jnp.where(band & (ik >= low), 0.0, NEG)
    mid_bias[1] = jnp.where(band & (ik < high), 0.0, NEG)
    iq, ik = iota((2 * SIDE, 6 * SIDE), 0), iota((2 * SIDE, 6 * SIDE), 1)
    vq = (iq >> 5) * BLK + (iq & 15)
    vk = (ik >> 5) * BLK + (ik & 15)
    band = (vk >= vq) & (vk <= vq + 2 * SIDE) & ((iq & 16) == (ik & 16))
    band = band & (vk >= first * SIDE) & (vk < (3 - last) * SIDE)
    far_bias[...] = jnp.where(band, 0.0, NEG)
    lead[...] = place[:, :HEAD_DIM]

    for h in range(heads):
        for k in PEERS:
            x_kv(h, k).wait_recv()
            y_each("start", [(h, k)], y_out)

    def near(h):
        cols = slice(h * HEAD_DIM, (h + 1) * HEAD_DIM)
        for b in range(2):
            span = slice(b * 2 * SIDE, (b + 1) * 2 * SIDE)
            keys = slice(b * 2 * SIDE, b * 2 * SIDE + 4 * SIDE)
            m, l, acc = attend(qn[span, cols], kn[keys, cols], vn[keys, cols], near_bias[b])
            nm[h, span] = m
            nl[h, span] = l
            nacc[h, span] = acc

    def give_back(h, k):
        s = xpeer(k)
        return [
            remote(sret.at[h, s], ret.at[h, x], rs.at[h, k, 0], rr.at[h, k, 0], (base + s, tp)),
            remote(sstat.at[h, s], rstat.at[h, x], rs.at[h, k, 1], rr.at[h, k, 1], (base + s, tp)),
        ]

    def residue(h):
        for k in PEERS:
            x_q(h, k).wait_recv()
        y_each("wait_recv", [(h, k) for k in range(ROW)], y_in)
        far, mid = [], []
        for e in range(2):
            two = slice(2 * e, 2 * e + 2)
            q = qres[h, :, two].reshape(2 * SIDE, HEAD_DIM)
            k = kvres[h, :, 0, two].reshape(6 * SIDE, HEAD_DIM)
            v = kvres[h, :, 1, two].reshape(6 * SIDE, HEAD_DIM)
            far.append(attend(q, k, v, far_bias[...]))
            q = qres[h, two].reshape(2 * SIDE, HEAD_DIM)
            k = kvres[h, 2 * e + 3 : 2 * e + 7, 0].reshape(4 * SIDE, HEAD_DIM)
            v = kvres[h, 2 * e + 3 : 2 * e + 7, 1].reshape(4 * SIDE, HEAD_DIM)
            mid.append(attend(q, k, v, mid_bias[e]))
        for s in range(ROW):
            part = slice(s % 2 * SIDE, (s % 2 + 1) * SIDE)
            m1, l1, acc1 = (mid[s // 2][i][part] for i in range(3))
            part = slice(s * 2 * BLK, (s + 1) * 2 * BLK)
            m2, l2, acc2 = (
                jnp.concatenate([f[i][part] for f in far], axis=0) for i in range(3)
            )
            m = jnp.maximum(m1, m2)
            a1, a2 = jnp.exp2(m1 - m), jnp.exp2(m2 - m)
            l = a1 * l1 + a2 * l2
            inv = 1.0 / l
            sret[h, s] = ((a1 * inv) * acc1 + (a2 * inv) * acc2).astype(BF)
            lse = jnp.broadcast_to(m + jnp.log2(l), (SIDE, HEAD_DIM))
            flat = jnp.transpose(jnp.concatenate([lse, lse], axis=0))
            sstat[h, s] = flat[:1]
        for k in PEERS:
            for copy in give_back(h, k):
                copy.start()
        ret[h, x] = sret[h, x]
        rstat[h, x] = sstat[h, x]

    def columns(h, side):
        return pl.ds(pl.multiple_of((side * heads + h) * HEAD_DIM, HEAD_DIM), HEAD_DIM)

    def tp_copy(h):
        mine = out_ref.at[:, columns(h, tp)]
        return remote(mine, mine, ts.at[h], tr.at[h], (sp, 1 - tp))

    def combine(h):
        for k in PEERS:
            for copy in give_back(h, k):
                copy.wait_recv()
        got = ret[h].reshape(rows, HEAD_DIM)
        out = jnp.dot(unperm, got, preferred_element_type=F32)
        lane = iota((rows, HEAD_DIM), 1)
        small = iota((1, HEAD_DIM), 1)
        where = lead[...]
        col = jnp.zeros((rows, HEAD_DIM), F32)
        for pair in range(2):
            row = jnp.where(
                small < piece, rstat[h, 2 * pair], rstat[h, 2 * pair + 1]
            )
            col = jnp.where(where == lane + pair * HEAD_DIM, row, col)
        lse = jnp.sum(col, axis=1, keepdims=True)
        m0 = nm[h]
        m = jnp.maximum(m0, lse)
        a0, a1 = jnp.exp2(m0 - m), jnp.exp2(lse - m)
        inv = 1.0 / (a0 * nl[h] + a1)
        att = (a0 * inv) * nacc[h] + (a1 * inv) * out
        out_ref[:, columns(h, tp)] = att.astype(BF)
        tp_copy(h).start()

    for h in range(heads):
        residue(h)
    halo("wait_recv", halo_in)
    for h in range(heads):
        near(h)
    for h in range(heads):
        combine(h)
    for h in range(heads):
        tp_copy(h).wait_recv()

    for h in range(heads):
        for k in PEERS:
            x_kv(h, k).wait_send()
            x_q(h, k).wait_send()
            for copy in give_back(h, k):
                copy.wait_send()
        y_each("wait_send", [(h, k) for k in range(ROW)], y_out)
        tp_copy(h).wait_send()
    halo("wait_send", halo_out)


def per_device(n, queries, keys, values, w_out):
    rows, columns = queries.shape
    heads = columns // HEAD_DIM
    vmem = pltpu.VMEM
    dma = pltpu.SemaphoreType.DMA
    attended = pl.pallas_call(
        functools.partial(kernel, n, heads),
        out_shape=jax.ShapeDtypeStruct((rows, 2 * columns), BF),
        in_specs=[pl.BlockSpec(memory_space=pl.ANY)] * 3,
        out_specs=pl.BlockSpec(memory_space=pltpu.VMEM),
        scratch_shapes=[
            vmem((rows, columns), BF),
            vmem((rows + 2 * SIDE, columns), BF),
            vmem((rows + 2 * SIDE, columns), BF),
            vmem((ROW, heads, 2, SUB, BLK, HEAD_DIM), BF),
            vmem((ROW, heads, SUB, BLK, HEAD_DIM), BF),
            vmem((heads, 3 * ROW, 2, SUB, BLK, HEAD_DIM), BF),
            vmem((heads, ROW, SUB, BLK, HEAD_DIM), BF),
            vmem((heads, ROW, SIDE, HEAD_DIM), BF),
            vmem((heads, ROW, 1, HEAD_DIM), F32),
            vmem((heads, ROW, SIDE, HEAD_DIM), BF),
            vmem((heads, ROW, 1, HEAD_DIM), F32),
            vmem((heads, rows, HEAD_DIM), F32),
            vmem((heads, rows, 1), F32),
            vmem((heads, rows, 1), F32),
            vmem((2, 2 * SIDE, 4 * SIDE), F32),
            vmem((2, 2 * SIDE, 4 * SIDE), F32),
            vmem((2 * SIDE, 6 * SIDE), F32),
            vmem((rows, HEAD_DIM), jnp.int32),
            dma((3,)),
            dma((heads, ROW, 2)),
            dma((heads, ROW, 2)),
            dma((heads, ROW, 2)),
            dma((heads, ROW, 2)),
            dma((2, 2)),
            dma((2, 2)),
            dma((heads, ROW, 2)),
            dma((heads, ROW, 2)),
            dma((heads,)),
            dma((heads,)),
        ],
        compiler_params=pltpu.CompilerParams(
            collective_id=0, has_side_effects=True, vmem_limit_bytes=20 * 1024 * 1024
        ),
        name="fused",
    )(queries, keys, values)
    return jnp.dot(attended, w_out, preferred_element_type=F32).astype(BF)


def solution(mesh):
    return jax.shard_map(
        functools.partial(per_device, mesh.shape["sp"]),
        mesh=mesh,
        in_specs=(P("sp", "tp"), P("sp", "tp"), P("sp", "tp"), P(None, "tp")),
        out_specs=P("sp", "tp"),
        check_vma=False,
    )
```

```python
import functools
import math

import jax
import jax.numpy as jnp
from jax import lax
from jax.experimental import pallas as pl
from jax.experimental.pallas import tpu as pltpu
from jax.sharding import PartitionSpec as P

HEAD_DIM = 128
SIDE = 64
ROW = 4
SUB = 4
BLK = 16
MESH = pl.DeviceIdType.MESH
scope = jax.named_scope
BF, F32 = jnp.bfloat16, jnp.float32
NEG = -1e30
COEF = math.log2(math.e) / math.sqrt(HEAD_DIM)
PEERS = (1, 3, 2)


def attend(q, k, v, bias):
    s = lax.dot_general(q, k, (((1,), (1,)), ((), ())), preferred_element_type=F32)
    t = s * COEF + bias
    m = jnp.max(t, axis=1, keepdims=True)
    p = jnp.exp2(t - m)
    l = jnp.sum(p, axis=1, keepdims=True)
    acc = jnp.dot(p.astype(BF), v, preferred_element_type=F32)
    return m, l, acc


def kernel(
    n, heads, q_hbm, k_hbm, v_hbm, out_ref,
    qn, kn, vn, xkv, xq, kvres, qres, sret, sstat, ret, rstat,
    nacc, nm, nl, near_bias, mid_bias, far_bias, lead,
    lsem, xs, xr, qr, ys, yr, ns, nr, rs, rr, ts,
):
    sp, tp = lax.axis_index("sp"), lax.axis_index("tp")
    x = lax.rem(sp, ROW)
    base = sp - x
    up = lax.rem(sp + ROW, n)
    down = lax.rem(sp + n - ROW, n)
    right = lax.rem(sp + 1, n)
    left = lax.rem(sp + n - 1, n)
    rows = qn.shape[0]
    piece = rows // ROW

    loads = [
        pltpu.make_async_copy(k_hbm, kn.at[pl.ds(SIDE, rows)], lsem.at[0]),
        pltpu.make_async_copy(v_hbm, vn.at[pl.ds(SIDE, rows)], lsem.at[1]),
        pltpu.make_async_copy(q_hbm, qn, lsem.at[2]),
    ]
    for copy in loads:
        copy.start()

    def xpeer(k):
        return lax.rem(x + k, ROW)

    first = (sp < ROW).astype(jnp.int32)
    last = (sp >= n - ROW).astype(jnp.int32)
    start = (sp == 0).astype(jnp.int32)
    end = (sp == n - 1).astype(jnp.int32)
    to_up, to_down, to_right, to_left = sp < n - ROW, sp >= ROW, sp < n - 1, sp >= 1

    barrier = pltpu.get_barrier_semaphore()

    def greet(friend):
        pl.semaphore_signal(barrier, inc=1, device_id=friend, device_id_type=MESH)

    for k in PEERS:
        greet((base + xpeer(k), tp))
    greet((sp, 1 - tp))
    pl.when(to_up)(lambda: greet((up, tp)))
    pl.when(to_down)(lambda: greet((down, tp)))
    pl.when(to_right)(lambda: greet((right, tp)))
    pl.when(to_left)(lambda: greet((left, tp)))

    def iota(shape, dim):
        return lax.broadcasted_iota(jnp.int32, shape, dim)

    r, t = iota((rows, rows), 0), iota((rows, rows), 1)
    order = (r & 15) * 16 + ((r >> 4) & 3) * 4 + (r >> 6)
    perm = jnp.where(t == order, 1.0, 0.0).astype(BF)
    place = (r & 3) * 64 + ((r >> 2) & 3) * 16 + (r >> 4)
    unperm = jnp.where(t == place, 1.0, 0.0).astype(BF)

    with scope("load_k"):
        loads[0].wait()
    kp = jnp.dot(perm, kn[SIDE : SIDE + rows], preferred_element_type=F32).astype(BF)
    with scope("load_v"):
        loads[1].wait()
    vp = jnp.dot(perm, vn[SIDE : SIDE + rows], preferred_element_type=F32).astype(BF)

    def cut(a, c, h):
        a = a[c * piece : (c + 1) * piece, h * HEAD_DIM : (h + 1) * HEAD_DIM]
        return a.reshape(SUB, BLK, HEAD_DIM)

    for h in range(heads):
        for c in range(ROW):
            xkv[c, h, 0] = cut(kp, c, h)
            xkv[c, h, 1] = cut(vp, c, h)

    with scope("barrier"):
        pl.semaphore_wait(barrier, 2 * ROW - first - last - start - end)

    def remote(src, dst, ssem, rsem, device):
        return pltpu.make_async_remote_copy(
            src_ref=src, dst_ref=dst, send_sem=ssem, recv_sem=rsem,
            device_id=device, device_id_type=MESH,
        )

    def x_kv(h, k):
        c = xpeer(k)
        return remote(
            xkv.at[c, h], kvres.at[h, ROW + x], xs.at[0], xr.at[h, k - 1], (base + c, tp)
        )

    def x_q(h, k):
        c = xpeer(k)
        return remote(xq.at[c, h], qres.at[h, x], xs.at[1], qr.at[h], (base + c, tp))

    def y_kv(h, k, way):
        s = xpeer(ROW - k)
        region = 0 if way == 0 else 2 * ROW
        return remote(
            xkv.at[x, h] if k == 0 else kvres.at[h, ROW + s], kvres.at[h, region + s],
            ys.at[way], yr.at[h, way], (up if way == 0 else down, tp),
        )

    def taken(ref, sem):
        remote(ref, ref, sem, sem, (sp, 1 - tp)).wait_recv()

    def y_send(pairs):
        for way, side in enumerate(y_out):
            @pl.when(side)
            def _():
                for h, k in pairs:
                    y_kv(h, k, way).start()

    def y_wait(h):
        for way, side in enumerate(y_in):
            @pl.when(side)
            def _():
                taken(kvres.at[h, pl.ds(0, ROW)], yr.at[h, way])

    def halo_send():
        for way, side in enumerate(halo_out):
            @pl.when(side)
            def _():
                for a in (kn, vn):
                    if way == 0:
                        src, dst, who = pl.ds(rows, SIDE), pl.ds(0, SIDE), right
                    else:
                        src, dst, who = pl.ds(SIDE, SIDE), pl.ds(SIDE + rows, SIDE), left
                    remote(a.at[src], a.at[dst], ns.at[way], nr.at[way], (who, tp)).start()

    def halo_wait(sems, sides):
        for way, side in enumerate(sides):
            @pl.when(side)
            def _():
                taken(kn.at[pl.ds(0, 2 * SIDE)], sems.at[way])

    y_out, y_in = (to_up, to_down), (to_down, to_up)
    halo_out, halo_in = (to_right, to_left), (to_left, to_right)

    for h in range(heads):
        for k in PEERS:
            x_kv(h, k).start()
    y_send([(h, 0) for h in range(heads)])
    with scope("load_q"):
        loads[2].wait()
    qp = jnp.dot(perm, qn[...], preferred_element_type=F32).astype(BF)
    for h in range(heads):
        for c in range(ROW):
            xq[c, h] = cut(qp, c, h)
    for h in range(heads):
        for k in PEERS:
            x_q(h, k).start()
    for h in range(heads):
        kvres[h, ROW + x] = xkv[x, h]
        qres[h, x] = xq[x, h]

    blank = jnp.zeros((heads, ROW, 2, SUB, BLK, HEAD_DIM), BF)
    edge = jnp.zeros((SIDE, heads * HEAD_DIM), BF)

    @pl.when(sp < ROW)
    def _():
        kvres[:, :ROW] = blank

    @pl.when(sp >= n - ROW)
    def _():
        kvres[:, 2 * ROW :] = blank

    @pl.when(sp == 0)
    def _():
        kn[:SIDE] = edge
        vn[:SIDE] = edge

    @pl.when(sp == n - 1)
    def _():
        kn[SIDE + rows :] = edge
        vn[SIDE + rows :] = edge

    iq, ik = iota((2 * SIDE, 4 * SIDE), 0), iota((2 * SIDE, 4 * SIDE), 1)
    band = (ik >= iq) & (ik <= iq + 2 * SIDE)
    near_bias[0] = jnp.where(band & (ik >= start * SIDE), 0.0, NEG)
    near_bias[1] = jnp.where(band & (ik < 4 * SIDE - end * SIDE), 0.0, NEG)
    low, high = first * SIDE, (4 - last) * SIDE
    wq = (iq >> 6) * 64 + (iq & 15) * 4 + ((iq >> 4) & 3)
    wk = (ik >> 6) * 64 - SIDE + (ik & 15) * 4 + ((ik >> 4) & 3)
    band = (wk - wq <= SIDE) & (wq - wk <= SIDE)
    mid_bias[0] = jnp.where(band & (ik >= low), 0.0, NEG)
    mid_bias[1] = jnp.where(band & (ik < high), 0.0, NEG)
    iq, ik = iota((2 * SIDE, 6 * SIDE), 0), iota((2 * SIDE, 6 * SIDE), 1)
    vq = (iq >> 5) * BLK + (iq & 15)
    vk = (ik >> 5) * BLK + (ik & 15)
    band = (vk >= vq) & (vk <= vq + 2 * SIDE) & ((iq & 16) == (ik & 16))
    band = band & (vk >= first * SIDE) & (vk < (3 - last) * SIDE)
    far_bias[...] = jnp.where(band, 0.0, NEG)
    lead[...] = place[:, :HEAD_DIM]

    def relay(h):
        for k in PEERS:
            with scope(f"relay_{h}_{k}"):
                x_kv(h, k).wait_recv()
            y_send([(h, k)])

    def near(h):
        cols = slice(h * HEAD_DIM, (h + 1) * HEAD_DIM)
        for b in range(2):
            span = slice(b * 2 * SIDE, (b + 1) * 2 * SIDE)
            keys = slice(b * 2 * SIDE, b * 2 * SIDE + 4 * SIDE)
            m, l, acc = attend(qn[span, cols], kn[keys, cols], vn[keys, cols], near_bias[b])
            nm[h, span] = m
            nl[h, span] = l
            nacc[h, span] = acc

    def give_back(h, k):
        s = xpeer(k)
        return [
            remote(sret.at[h, s], ret.at[h, x], rs.at[0], rr.at[h, 0], (base + s, tp)),
            remote(sstat.at[h, s], rstat.at[h, x], rs.at[1], rr.at[h, 1], (base + s, tp)),
        ]

    def residue(h):
        with scope(f"wait_q_{h}"):
            taken(qres.at[h, pl.ds(0, ROW - 1)], qr.at[h])
        with scope(f"wait_y_{h}"):
            y_wait(h)
        far, mid = [], []
        for e in range(2):
            two = slice(2 * e, 2 * e + 2)
            q = qres[h, :, two].reshape(2 * SIDE, HEAD_DIM)
            k = kvres[h, :, 0, two].reshape(6 * SIDE, HEAD_DIM)
            v = kvres[h, :, 1, two].reshape(6 * SIDE, HEAD_DIM)
            far.append(attend(q, k, v, far_bias[...]))
            q = qres[h, two].reshape(2 * SIDE, HEAD_DIM)
            k = kvres[h, 2 * e + 3 : 2 * e + 7, 0].reshape(4 * SIDE, HEAD_DIM)
            v = kvres[h, 2 * e + 3 : 2 * e + 7, 1].reshape(4 * SIDE, HEAD_DIM)
            mid.append(attend(q, k, v, mid_bias[e]))
        for s in range(ROW):
            part = slice(s % 2 * SIDE, (s % 2 + 1) * SIDE)
            m1, l1, acc1 = (mid[s // 2][i][part] for i in range(3))
            part = slice(s * 2 * BLK, (s + 1) * 2 * BLK)
            m2, l2, acc2 = (
                jnp.concatenate([f[i][part] for f in far], axis=0) for i in range(3)
            )
            m = jnp.maximum(m1, m2)
            a1, a2 = jnp.exp2(m1 - m), jnp.exp2(m2 - m)
            l = a1 * l1 + a2 * l2
            inv = 1.0 / l
            sret[h, s] = ((a1 * inv) * acc1 + (a2 * inv) * acc2).astype(BF)
            lse = jnp.broadcast_to(m + jnp.log2(l), (SIDE, HEAD_DIM))
            flat = jnp.transpose(jnp.concatenate([lse, lse], axis=0))
            sstat[h, s] = flat[:1]
        for k in PEERS:
            for copy in give_back(h, k):
                copy.start()
        ret[h, x] = sret[h, x]
        rstat[h, x] = sstat[h, x]

    def columns(h, side):
        return pl.ds(pl.multiple_of((side * heads + h) * HEAD_DIM, HEAD_DIM), HEAD_DIM)

    def tp_copy(h):
        mine = out_ref.at[:, columns(h, tp)]
        return remote(mine, mine, ts.at[0], ts.at[1], (sp, 1 - tp))

    def combine(h):
        with scope(f"wait_back_{h}"):
            taken(ret.at[h, pl.ds(0, ROW - 1)], rr.at[h, 0])
            taken(rstat.at[h, pl.ds(0, ROW - 1)], rr.at[h, 1])
        got = ret[h].reshape(rows, HEAD_DIM)
        out = jnp.dot(unperm, got, preferred_element_type=F32)
        lane = iota((rows, HEAD_DIM), 1)
        small = iota((1, HEAD_DIM), 1)
        where = lead[...]
        col = jnp.zeros((rows, HEAD_DIM), F32)
        for pair in range(2):
            row = jnp.where(
                small < piece, rstat[h, 2 * pair], rstat[h, 2 * pair + 1]
            )
            col = jnp.where(where == lane + pair * HEAD_DIM, row, col)
        lse = jnp.sum(col, axis=1, keepdims=True)
        m0 = nm[h]
        m = jnp.maximum(m0, lse)
        a0, a1 = jnp.exp2(m0 - m), jnp.exp2(lse - m)
        inv = 1.0 / (a0 * nl[h] + a1)
        att = (a0 * inv) * nacc[h] + (a1 * inv) * out
        out_ref[:, columns(h, tp)] = att.astype(BF)
        tp_copy(h).start()

    relay(0)
    relay(1)
    relay(2)
    residue(0)
    relay(3)
    halo_send()
    residue(1)
    residue(2)
    residue(3)
    with scope("wait_halo"):
        halo_wait(nr, halo_in)
    for h in range(heads):
        near(h)
    for h in range(heads):
        combine(h)

    with scope("send_waits"):
        taken(xkv.at[pl.ds(0, ROW - 1)], xs.at[0])
        taken(xq.at[pl.ds(0, ROW - 1)], xs.at[1])
        for way, side in enumerate(y_out):
            @pl.when(side)
            def _():
                taken(xkv, ys.at[way])
        halo_wait(ns, halo_out)
        taken(sret.at[:, pl.ds(0, ROW - 1)], rs.at[0])
        taken(sstat.at[:, pl.ds(0, ROW - 1)], rs.at[1])
    with scope("wait_tp"):
        taken(qn, ts.at[1])
        taken(qn, ts.at[0])


def per_device(n, queries, keys, values, w_out):
    rows, columns = queries.shape
    heads = columns // HEAD_DIM
    vmem = pltpu.VMEM
    dma = pltpu.SemaphoreType.DMA
    attended = pl.pallas_call(
        functools.partial(kernel, n, heads),
        out_shape=jax.ShapeDtypeStruct((rows, 2 * columns), BF),
        in_specs=[pl.BlockSpec(memory_space=pltpu.HBM)] * 3,
        out_specs=pl.BlockSpec(memory_space=pltpu.VMEM),
        scratch_shapes=[
            vmem((rows, columns), BF),
            vmem((rows + 2 * SIDE, columns), BF),
            vmem((rows + 2 * SIDE, columns), BF),
            vmem((ROW, heads, 2, SUB, BLK, HEAD_DIM), BF),
            vmem((ROW, heads, SUB, BLK, HEAD_DIM), BF),
            vmem((heads, 3 * ROW, 2, SUB, BLK, HEAD_DIM), BF),
            vmem((heads, ROW, SUB, BLK, HEAD_DIM), BF),
            vmem((heads, ROW, SIDE, HEAD_DIM), BF),
            vmem((heads, ROW, 1, HEAD_DIM), F32),
            vmem((heads, ROW, SIDE, HEAD_DIM), BF),
            vmem((heads, ROW, 1, HEAD_DIM), F32),
            vmem((heads, rows, HEAD_DIM), F32),
            vmem((heads, rows, 1), F32),
            vmem((heads, rows, 1), F32),
            vmem((2, 2 * SIDE, 4 * SIDE), F32),
            vmem((2, 2 * SIDE, 4 * SIDE), F32),
            vmem((2 * SIDE, 6 * SIDE), F32),
            vmem((rows, HEAD_DIM), jnp.int32),
            dma((3,)),
            dma((2,)),
            dma((heads, ROW - 1)),
            dma((heads,)),
            dma((2,)),
            dma((heads, 2)),
            dma((2,)),
            dma((2,)),
            dma((2,)),
            dma((heads, 2)),
            dma((2,)),
        ],
        compiler_params=pltpu.CompilerParams(
            collective_id=0, has_side_effects=True, vmem_limit_bytes=20 * 1024 * 1024
        ),
        name="fused",
    )(*(pltpu.with_memory_space_constraint(a, pltpu.HBM) for a in (queries, keys, values)))
    return jnp.dot(attended, w_out, preferred_element_type=F32).astype(BF)


def solution(mesh):
    return jax.shard_map(
        functools.partial(per_device, mesh.shape["sp"]),
        mesh=mesh,
        in_specs=(P("sp", "tp"), P("sp", "tp"), P("sp", "tp"), P(None, "tp")),
        out_specs=P("sp", "tp"),
        check_vma=False,
    )
```

```python
import functools
import math

import jax
import jax.numpy as jnp
from jax import lax
from jax.experimental import pallas as pl
from jax.experimental.pallas import tpu as pltpu
from jax.sharding import PartitionSpec as P

HEAD_DIM = 128
SIDE = 64
ROW = 4
SUB = 4
BLK = 16
MESH = pl.DeviceIdType.MESH
scope = jax.named_scope
BF, F32 = jnp.bfloat16, jnp.float32
NEG = -1e30
COEF = math.log2(math.e) / math.sqrt(HEAD_DIM)
PEERS = (1, 3, 2)
SENDS = (2, 1, 3)


def attend(q, k, v, bias):
    s = lax.dot_general(q, k, (((1,), (1,)), ((), ())), preferred_element_type=F32)
    t = s * COEF + bias
    m = jnp.max(t, axis=1, keepdims=True)
    p = jnp.exp2(t - m)
    l = jnp.sum(p, axis=1, keepdims=True)
    acc = jnp.dot(p.astype(BF), v, preferred_element_type=F32)
    return jnp.broadcast_to(m, acc.shape), jnp.broadcast_to(l, acc.shape), acc


def kernel(
    n, heads, q_hbm, k_hbm, v_hbm, out_ref,
    qn, kn, vn, xkv, xq, kvres, qres, sret, sstat, ret, rstat,
    nacc, nm, nl, near_bias, mid_bias, far_bias, lead,
    lsem, xs, xr, qr, ys, yr, ns, nr, rs, rr, ts,
):
    sp, tp = lax.axis_index("sp"), lax.axis_index("tp")
    x = lax.rem(sp, ROW)
    base = sp - x
    up = lax.rem(sp + ROW, n)
    down = lax.rem(sp + n - ROW, n)
    right = lax.rem(sp + 1, n)
    left = lax.rem(sp + n - 1, n)
    rows = qn.shape[0]
    piece = rows // ROW

    loads = [
        pltpu.make_async_copy(k_hbm, kn.at[pl.ds(SIDE, rows)], lsem.at[0]),
        pltpu.make_async_copy(v_hbm, vn.at[pl.ds(SIDE, rows)], lsem.at[1]),
        pltpu.make_async_copy(q_hbm, qn, lsem.at[2]),
    ]
    for copy in loads:
        copy.start()

    def xpeer(k):
        return lax.rem(x + k, ROW)

    first = (sp < ROW).astype(jnp.int32)
    last = (sp >= n - ROW).astype(jnp.int32)
    start = (sp == 0).astype(jnp.int32)
    end = (sp == n - 1).astype(jnp.int32)
    to_up, to_down, to_right, to_left = sp < n - ROW, sp >= ROW, sp < n - 1, sp >= 1

    barrier = pltpu.get_barrier_semaphore()

    def greet(friend):
        pl.semaphore_signal(barrier, inc=1, device_id=friend, device_id_type=MESH)

    for k in PEERS:
        greet((base + xpeer(k), tp))
    greet((sp, 1 - tp))
    pl.when(to_up)(lambda: greet((up, tp)))
    pl.when(to_down)(lambda: greet((down, tp)))
    pl.when(to_right)(lambda: greet((right, tp)))
    pl.when(to_left)(lambda: greet((left, tp)))

    def iota(shape, dim):
        return lax.broadcasted_iota(jnp.int32, shape, dim)

    r, t = iota((rows, rows), 0), iota((rows, rows), 1)
    order = (r & 15) * 16 + ((r >> 4) & 3) * 4 + (r >> 6)
    perm = jnp.where(t == order, 1.0, 0.0).astype(BF)
    place = (r & 3) * 64 + ((r >> 2) & 3) * 16 + (r >> 4)
    unperm = jnp.where(t == place, 1.0, 0.0).astype(BF)

    with scope("load_k"):
        loads[0].wait()
    kp = jnp.dot(perm, kn[SIDE : SIDE + rows], preferred_element_type=F32).astype(BF)
    with scope("load_v"):
        loads[1].wait()
    vp = jnp.dot(perm, vn[SIDE : SIDE + rows], preferred_element_type=F32).astype(BF)

    def cut(a, c, h):
        a = a[c * piece : (c + 1) * piece, h * HEAD_DIM : (h + 1) * HEAD_DIM]
        return a.reshape(SUB, BLK, HEAD_DIM)

    for h in range(heads):
        for c in range(ROW):
            xkv[c, h, 0] = cut(kp, c, h)
            xkv[c, h, 1] = cut(vp, c, h)

    with scope("barrier"):
        pl.semaphore_wait(barrier, 2 * ROW - first - last - start - end)

    def remote(src, dst, ssem, rsem, device):
        return pltpu.make_async_remote_copy(
            src_ref=src, dst_ref=dst, send_sem=ssem, recv_sem=rsem,
            device_id=device, device_id_type=MESH,
        )

    def x_kv(h, k):
        c = xpeer(k)
        return remote(
            xkv.at[c, h], kvres.at[h, ROW + x], xs.at[0], xr.at[h, k - 1], (base + c, tp)
        )

    def x_q(h, k):
        c = xpeer(k)
        return remote(xq.at[c, h], qres.at[h, x], xs.at[1], qr.at[h], (base + c, tp))

    def y_kv(h, k, way):
        s = xpeer(ROW - k)
        region = 0 if way == 0 else 2 * ROW
        return remote(
            xkv.at[x, h] if k == 0 else kvres.at[h, ROW + s], kvres.at[h, region + s],
            ys.at[way], yr.at[h, way], (up if way == 0 else down, tp),
        )

    def taken(ref, sem):
        remote(ref, ref, sem, sem, (sp, 1 - tp)).wait_recv()

    def y_send(pairs):
        for way, side in enumerate(y_out):
            @pl.when(side)
            def _():
                for h, k in pairs:
                    y_kv(h, k, way).start()

    def y_wait(h):
        for way, side in enumerate(y_in):
            @pl.when(side)
            def _():
                taken(kvres.at[h, pl.ds(0, ROW)], yr.at[h, way])

    def halo_send(sides):
        for way, side in enumerate(sides):
            @pl.when(side)
            def _():
                for a in (kn, vn):
                    if way == 0:
                        src, dst, who = pl.ds(rows, SIDE), pl.ds(0, SIDE), right
                    else:
                        src, dst, who = pl.ds(SIDE, SIDE), pl.ds(SIDE + rows, SIDE), left
                    remote(a.at[src], a.at[dst], ns.at[way], nr.at[way], (who, tp)).start()

    def halo_wait(sems, sides):
        for way, side in enumerate(sides):
            @pl.when(side)
            def _():
                taken(kn.at[pl.ds(0, 2 * SIDE)], sems.at[way])

    y_out, y_in = (to_up, to_down), (to_down, to_up)
    halo_out, halo_in = (to_right, to_left), (to_left, to_right)

    for h in range(heads - 1):
        for k in SENDS:
            x_kv(h, k).start()
    y_send([(h, 0) for h in range(heads)])
    with scope("load_q"):
        loads[2].wait()
    qp = jnp.dot(perm, qn[...], preferred_element_type=F32).astype(BF)
    for h in range(heads):
        for c in range(ROW):
            xq[c, h] = cut(qp, c, h)
    for h in range(heads):
        for k in SENDS:
            x_q(h, k).start()
        if h == 0:
            for k in SENDS:
                x_kv(heads - 1, k).start()
    halo_send((to_right & (x < ROW - 1), to_left & (x > 0)))
    for h in range(heads):
        kvres[h, ROW + x] = xkv[x, h]
        qres[h, x] = xq[x, h]

    blank = jnp.zeros((heads, ROW, 2, SUB, BLK, HEAD_DIM), BF)
    edge = jnp.zeros((SIDE, heads * HEAD_DIM), BF)

    @pl.when(sp < ROW)
    def _():
        kvres[:, :ROW] = blank

    @pl.when(sp >= n - ROW)
    def _():
        kvres[:, 2 * ROW :] = blank

    @pl.when(sp == 0)
    def _():
        kn[:SIDE] = edge
        vn[:SIDE] = edge

    @pl.when(sp == n - 1)
    def _():
        kn[SIDE + rows :] = edge
        vn[SIDE + rows :] = edge

    iq, ik = iota((2 * SIDE, 4 * SIDE), 0), iota((2 * SIDE, 4 * SIDE), 1)
    band = (ik >= iq) & (ik <= iq + 2 * SIDE)
    near_bias[0] = jnp.where(band & (ik >= start * SIDE), 0.0, NEG)
    near_bias[1] = jnp.where(band & (ik < 4 * SIDE - end * SIDE), 0.0, NEG)
    low, high = first * SIDE, (4 - last) * SIDE
    wq = (iq >> 6) * 64 + (iq & 15) * 4 + ((iq >> 4) & 3)
    wk = (ik >> 6) * 64 - SIDE + (ik & 15) * 4 + ((ik >> 4) & 3)
    band = (wk - wq <= SIDE) & (wq - wk <= SIDE)
    mid_bias[0] = jnp.where(band & (ik >= low), 0.0, NEG)
    mid_bias[1] = jnp.where(band & (ik < high), 0.0, NEG)
    iq, ik = iota((2 * SIDE, 6 * SIDE), 0), iota((2 * SIDE, 6 * SIDE), 1)
    vq = (iq >> 5) * BLK + (iq & 15)
    vk = (ik >> 5) * BLK + (ik & 15)
    band = (vk >= vq) & (vk <= vq + 2 * SIDE) & ((iq & 16) == (ik & 16))
    band = band & (vk >= first * SIDE) & (vk < (3 - last) * SIDE)
    far_bias[...] = jnp.where(band, 0.0, NEG)
    lead[...] = place[:, :HEAD_DIM]

    def relay(h):
        for k in PEERS:
            with scope(f"relay_{h}_{k}"):
                x_kv(h, k).wait_recv()
            y_send([(h, k)])

    def near(h):
        cols = slice(h * HEAD_DIM, (h + 1) * HEAD_DIM)
        for b in range(2):
            span = slice(b * 2 * SIDE, (b + 1) * 2 * SIDE)
            keys = slice(b * 2 * SIDE, b * 2 * SIDE + 4 * SIDE)
            m, l, acc = attend(qn[span, cols], kn[keys, cols], vn[keys, cols], near_bias[b])
            nm[h, span] = m
            nl[h, span] = l
            nacc[h, span] = acc

    def give_back(h, k):
        s = xpeer(k)
        return [
            remote(sret.at[h, s], ret.at[h, x], rs.at[0], rr.at[h, 0], (base + s, tp)),
            remote(sstat.at[h, s], rstat.at[h, x], rs.at[1], rr.at[h, 1], (base + s, tp)),
        ]

    def residue_wait(h):
        with scope(f"wait_q_{h}"):
            taken(qres.at[h, pl.ds(0, ROW - 1)], qr.at[h])
        with scope(f"wait_y_{h}"):
            y_wait(h)

    def residue_work(h):
        far, mid = [], []
        for e in range(2):
            two = slice(2 * e, 2 * e + 2)
            q = qres[h, :, two].reshape(2 * SIDE, HEAD_DIM)
            k = kvres[h, :, 0, two].reshape(6 * SIDE, HEAD_DIM)
            v = kvres[h, :, 1, two].reshape(6 * SIDE, HEAD_DIM)
            far.append(attend(q, k, v, far_bias[...]))
            q = qres[h, two].reshape(2 * SIDE, HEAD_DIM)
            k = kvres[h, 2 * e + 3 : 2 * e + 7, 0].reshape(4 * SIDE, HEAD_DIM)
            v = kvres[h, 2 * e + 3 : 2 * e + 7, 1].reshape(4 * SIDE, HEAD_DIM)
            mid.append(attend(q, k, v, mid_bias[e]))
        lses = []
        for s in range(ROW):
            part = slice(s % 2 * SIDE, (s % 2 + 1) * SIDE)
            m1, l1, acc1 = (mid[s // 2][i][part] for i in range(3))
            part = slice(s * 2 * BLK, (s + 1) * 2 * BLK)
            m2, l2, acc2 = (
                jnp.concatenate([f[i][part] for f in far], axis=0) for i in range(3)
            )
            m = jnp.maximum(m1, m2)
            a1, a2 = jnp.exp2(m1 - m), jnp.exp2(m2 - m)
            l = a1 * l1 + a2 * l2
            sret[h, s] = ((a1 * acc1 + a2 * acc2) / l).astype(BF)
            lses.append(m + jnp.log2(l))
        for e in range(2):
            flat = jnp.transpose(jnp.concatenate(lses[2 * e : 2 * e + 2], axis=0))
            sstat[h, 2 * e] = flat[:1]
            sstat[h, 2 * e + 1] = flat[:1]

    def residue(*which):
        for h in which:
            residue_wait(h)
        for h in which:
            residue_work(h)
        for h in which:
            for k in SENDS:
                for copy in give_back(h, k):
                    copy.start()
        for h in which:
            ret[h, x] = sret[h, x]
            rstat[h, x] = sstat[h, x]

    def columns(h, side):
        return pl.ds(pl.multiple_of((side * heads + h) * HEAD_DIM, HEAD_DIM), HEAD_DIM)

    def tp_copy(h):
        mine = out_ref.at[:, columns(h, tp)]
        return remote(mine, mine, ts.at[0], ts.at[1], (sp, 1 - tp))

    def combine(h):
        with scope(f"wait_back_{h}"):
            taken(ret.at[h, pl.ds(0, ROW - 1)], rr.at[h, 0])
            taken(rstat.at[h, pl.ds(0, ROW - 1)], rr.at[h, 1])
        got = ret[h].reshape(rows, HEAD_DIM)
        out = jnp.dot(unperm, got, preferred_element_type=F32)
        lane = iota((rows, HEAD_DIM), 1)
        small = iota((1, HEAD_DIM), 1)
        odd = jnp.broadcast_to(x & 1, (1, HEAD_DIM)) == 1
        where = lead[...]
        col = jnp.zeros((rows, HEAD_DIM), F32)
        for pair in range(2):
            one, two = rstat[h, 2 * pair], rstat[h, 2 * pair + 1]
            one = jnp.where(odd, pltpu.roll(one, SIDE, 1), one)
            two = jnp.where(odd, two, pltpu.roll(two, SIDE, 1))
            row = jnp.where(small < piece, one, two)
            col = jnp.where(where == lane + pair * HEAD_DIM, row, col)
        lse = jnp.broadcast_to(jnp.sum(col, axis=1, keepdims=True), col.shape)
        m0 = nm[h]
        m = jnp.maximum(m0, lse)
        a0, a1 = jnp.exp2(m0 - m), jnp.exp2(lse - m)
        att = (a0 * nacc[h] + a1 * out) / (a0 * nl[h] + a1)
        out_ref[:, columns(h, tp)] = att.astype(BF)
        tp_copy(h).start()

    relay(0)
    relay(1)
    relay(2)
    relay(3)
    halo_send((to_right & (x == ROW - 1), to_left & (x == 0)))
    for h in range(heads):
        residue(h)
    with scope("wait_halo"):
        halo_wait(nr, halo_in)
    for h in range(heads):
        near(h)
    for h in range(heads):
        combine(h)

    with scope("send_waits"):
        taken(xkv.at[pl.ds(0, ROW - 1)], xs.at[0])
        taken(xq.at[pl.ds(0, ROW - 1)], xs.at[1])
        for way, side in enumerate(y_out):
            @pl.when(side)
            def _():
                taken(xkv, ys.at[way])
        halo_wait(ns, halo_out)
        taken(sret.at[:, pl.ds(0, ROW - 1)], rs.at[0])
        taken(sstat.at[:, pl.ds(0, ROW - 1)], rs.at[1])
    with scope("wait_tp"):
        taken(qn, ts.at[1])
        taken(qn, ts.at[0])


def per_device(n, queries, keys, values, w_out):
    rows, columns = queries.shape
    heads = columns // HEAD_DIM
    vmem = pltpu.VMEM
    dma = pltpu.SemaphoreType.DMA
    attended = pl.pallas_call(
        functools.partial(kernel, n, heads),
        out_shape=jax.ShapeDtypeStruct((rows, 2 * columns), BF),
        in_specs=[pl.BlockSpec(memory_space=pltpu.HBM)] * 3,
        out_specs=pl.BlockSpec(memory_space=pltpu.VMEM),
        scratch_shapes=[
            vmem((rows, columns), BF),
            vmem((rows + 2 * SIDE, columns), BF),
            vmem((rows + 2 * SIDE, columns), BF),
            vmem((ROW, heads, 2, SUB, BLK, HEAD_DIM), BF),
            vmem((ROW, heads, SUB, BLK, HEAD_DIM), BF),
            vmem((heads, 3 * ROW, 2, SUB, BLK, HEAD_DIM), BF),
            vmem((heads, ROW, SUB, BLK, HEAD_DIM), BF),
            vmem((heads, ROW, SIDE, HEAD_DIM), BF),
            vmem((heads, ROW, 1, HEAD_DIM), F32),
            vmem((heads, ROW, SIDE, HEAD_DIM), BF),
            vmem((heads, ROW, 1, HEAD_DIM), F32),
            vmem((heads, rows, HEAD_DIM), F32),
            vmem((heads, rows, HEAD_DIM), F32),
            vmem((heads, rows, HEAD_DIM), F32),
            vmem((2, 2 * SIDE, 4 * SIDE), F32),
            vmem((2, 2 * SIDE, 4 * SIDE), F32),
            vmem((2 * SIDE, 6 * SIDE), F32),
            vmem((rows, HEAD_DIM), jnp.int32),
            dma((3,)),
            dma((2,)),
            dma((heads, ROW - 1)),
            dma((heads,)),
            dma((2,)),
            dma((heads, 2)),
            dma((2,)),
            dma((2,)),
            dma((2,)),
            dma((heads, 2)),
            dma((2,)),
        ],
        compiler_params=pltpu.CompilerParams(
            collective_id=0, has_side_effects=True, vmem_limit_bytes=20 * 1024 * 1024
        ),
        name="fused",
    )(*(pltpu.with_memory_space_constraint(a, pltpu.HBM) for a in (queries, keys, values)))
    return jnp.dot(attended, w_out, preferred_element_type=F32).astype(BF)


def solution(mesh):
    return jax.shard_map(
        functools.partial(per_device, mesh.shape["sp"]),
        mesh=mesh,
        in_specs=(P("sp", "tp"), P("sp", "tp"), P("sp", "tp"), P(None, "tp")),
        out_specs=P("sp", "tp"),
        check_vma=False,
    )
```

```python
import functools
import math

import jax
import jax.numpy as jnp
from jax import lax
from jax.experimental import pallas as pl
from jax.experimental.pallas import tpu as pltpu
from jax.sharding import PartitionSpec as P

HEAD_DIM = 128
SIDE = 64
ROW = 4
SUB = 4
BLK = 16
MESH = pl.DeviceIdType.MESH
scope = jax.named_scope
BF, F32 = jnp.bfloat16, jnp.float32
NEG = -1e30
COEF = math.log2(math.e) / math.sqrt(HEAD_DIM)
PEERS = (1, 3, 2)
SENDS = (1, 3, 2)


def attend(q, k, v, bias):
    s = lax.dot_general(q, k, (((1,), (1,)), ((), ())), preferred_element_type=F32)
    t = s * COEF + bias
    m = jnp.max(t, axis=1, keepdims=True)
    p = jnp.exp2(t - m)
    l = jnp.sum(p, axis=1, keepdims=True)
    acc = jnp.dot(p.astype(BF), v, preferred_element_type=F32)
    return jnp.broadcast_to(m, acc.shape), jnp.broadcast_to(l, acc.shape), acc


def kernel(
    n, heads, q_hbm, k_hbm, v_hbm, out_ref,
    qn, kn, vn, xkv, xq, kvres, qres, sret, sstat, ret, rstat,
    nacc, nm, nl, near_bias, mid_bias, far_bias, lead,
    lsem, xs, xr, qr, ys, yr, ns, nr, rs, rr, ts,
):
    sp, tp = lax.axis_index("sp"), lax.axis_index("tp")
    x = lax.rem(sp, ROW)
    base = sp - x
    up = lax.rem(sp + ROW, n)
    down = lax.rem(sp + n - ROW, n)
    right = lax.rem(sp + 1, n)
    left = lax.rem(sp + n - 1, n)
    rows = qn.shape[0]
    piece = rows // ROW

    loads = [
        pltpu.make_async_copy(k_hbm, kn.at[pl.ds(SIDE, rows)], lsem.at[0]),
        pltpu.make_async_copy(v_hbm, vn.at[pl.ds(SIDE, rows)], lsem.at[1]),
        pltpu.make_async_copy(q_hbm, qn, lsem.at[2]),
    ]
    for copy in loads:
        copy.start()

    def xpeer(k):
        return lax.rem(x + k, ROW)

    first = (sp < ROW).astype(jnp.int32)
    last = (sp >= n - ROW).astype(jnp.int32)
    start = (sp == 0).astype(jnp.int32)
    end = (sp == n - 1).astype(jnp.int32)
    to_up, to_down, to_right, to_left = sp < n - ROW, sp >= ROW, sp < n - 1, sp >= 1

    barrier = pltpu.get_barrier_semaphore()

    def greet(friend):
        pl.semaphore_signal(barrier, inc=1, device_id=friend, device_id_type=MESH)

    for k in PEERS:
        greet((base + xpeer(k), tp))
    greet((sp, 1 - tp))
    pl.when(to_up)(lambda: greet((up, tp)))
    pl.when(to_down)(lambda: greet((down, tp)))
    pl.when(to_right)(lambda: greet((right, tp)))
    pl.when(to_left)(lambda: greet((left, tp)))

    def iota(shape, dim):
        return lax.broadcasted_iota(jnp.int32, shape, dim)

    r, t = iota((rows, rows), 0), iota((rows, rows), 1)
    order = (r & 15) * 16 + ((r >> 4) & 3) * 4 + (r >> 6)
    perm = jnp.where(t == order, 1.0, 0.0).astype(BF)
    place = (r & 3) * 64 + ((r >> 2) & 3) * 16 + (r >> 4)
    unperm = jnp.where(t == place, 1.0, 0.0).astype(BF)

    with scope("load_k"):
        loads[0].wait()
    kp = jnp.dot(perm, kn[SIDE : SIDE + rows], preferred_element_type=F32).astype(BF)
    with scope("load_v"):
        loads[1].wait()
    vp = jnp.dot(perm, vn[SIDE : SIDE + rows], preferred_element_type=F32).astype(BF)

    def cut(a, c, h):
        a = a[c * piece : (c + 1) * piece, h * HEAD_DIM : (h + 1) * HEAD_DIM]
        return a.reshape(SUB, BLK, HEAD_DIM)

    for h in range(heads):
        for c in range(ROW):
            xkv[c, h, 0] = cut(kp, c, h)
            xkv[c, h, 1] = cut(vp, c, h)

    with scope("barrier"):
        pl.semaphore_wait(barrier, 2 * ROW - first - last - start - end)

    def remote(src, dst, ssem, rsem, device):
        return pltpu.make_async_remote_copy(
            src_ref=src, dst_ref=dst, send_sem=ssem, recv_sem=rsem,
            device_id=device, device_id_type=MESH,
        )

    def x_kv(h, k):
        c = xpeer(k)
        return remote(
            xkv.at[c, h], kvres.at[h, ROW + x], xs.at[0], xr.at[h, k - 1], (base + c, tp)
        )

    def x_q(h, k):
        c = xpeer(k)
        return remote(xq.at[c, h], qres.at[h, x], xs.at[1], qr.at[h], (base + c, tp))

    def y_kv(h, k, way):
        s = xpeer(ROW - k)
        region = 0 if way == 0 else 2 * ROW
        return remote(
            xkv.at[x, h] if k == 0 else kvres.at[h, ROW + s], kvres.at[h, region + s],
            ys.at[way], yr.at[h, way], (up if way == 0 else down, tp),
        )

    def taken(ref, sem):
        remote(ref, ref, sem, sem, (sp, 1 - tp)).wait_recv()

    def y_send(pairs):
        for way, side in enumerate(y_out):
            @pl.when(side)
            def _():
                for h, k in pairs:
                    y_kv(h, k, way).start()

    def y_wait(h):
        for way, side in enumerate(y_in):
            @pl.when(side)
            def _():
                taken(kvres.at[h, pl.ds(0, ROW)], yr.at[h, way])

    def halo_send(sides):
        for way, side in enumerate(sides):
            @pl.when(side)
            def _():
                for a in (kn, vn):
                    if way == 0:
                        src, dst, who = pl.ds(rows, SIDE), pl.ds(0, SIDE), right
                    else:
                        src, dst, who = pl.ds(SIDE, SIDE), pl.ds(SIDE + rows, SIDE), left
                    remote(a.at[src], a.at[dst], ns.at[way], nr.at[way], (who, tp)).start()

    def halo_wait(sems, sides):
        for way, side in enumerate(sides):
            @pl.when(side)
            def _():
                taken(kn.at[pl.ds(0, 2 * SIDE)], sems.at[way])

    y_out, y_in = (to_up, to_down), (to_down, to_up)
    halo_out, halo_in = (to_right, to_left), (to_left, to_right)

    for h in range(heads - 1):
        for k in SENDS:
            x_kv(h, k).start()
    y_send([(h, 0) for h in range(heads)])
    with scope("load_q"):
        loads[2].wait()
    qp = jnp.dot(perm, qn[...], preferred_element_type=F32).astype(BF)
    for h in range(heads):
        for c in range(ROW):
            xq[c, h] = cut(qp, c, h)
    for h in range(heads):
        for k in SENDS:
            x_q(h, k).start()
        if h == 0:
            for k in SENDS:
                x_kv(heads - 1, k).start()
    halo_send((to_right & (x < ROW - 1), to_left & (x > 0)))
    for h in range(heads):
        kvres[h, ROW + x] = xkv[x, h]
        qres[h, x] = xq[x, h]

    blank = jnp.zeros((heads, ROW, 2, SUB, BLK, HEAD_DIM), BF)
    edge = jnp.zeros((SIDE, heads * HEAD_DIM), BF)

    @pl.when(sp < ROW)
    def _():
        kvres[:, :ROW] = blank

    @pl.when(sp >= n - ROW)
    def _():
        kvres[:, 2 * ROW :] = blank

    @pl.when(sp == 0)
    def _():
        kn[:SIDE] = edge
        vn[:SIDE] = edge

    @pl.when(sp == n - 1)
    def _():
        kn[SIDE + rows :] = edge
        vn[SIDE + rows :] = edge

    iq, ik = iota((2 * SIDE, 4 * SIDE), 0), iota((2 * SIDE, 4 * SIDE), 1)
    band = (ik >= iq) & (ik <= iq + 2 * SIDE)
    near_bias[0] = jnp.where(band & (ik >= start * SIDE), 0.0, NEG)
    near_bias[1] = jnp.where(band & (ik < 4 * SIDE - end * SIDE), 0.0, NEG)
    low, high = first * SIDE, (4 - last) * SIDE
    wq = (iq >> 6) * 64 + (iq & 15) * 4 + ((iq >> 4) & 3)
    wk = (ik >> 6) * 64 - SIDE + (ik & 15) * 4 + ((ik >> 4) & 3)
    band = (wk - wq <= SIDE) & (wq - wk <= SIDE)
    mid_bias[0] = jnp.where(band & (ik >= low), 0.0, NEG)
    mid_bias[1] = jnp.where(band & (ik < high), 0.0, NEG)
    iq = iq & (SIDE - 1)
    band = (ik >= iq) & (ik <= iq + 2 * SIDE)
    band = band & (ik >= first * SIDE) & (ik < (3 - last) * SIDE)
    far_bias[...] = jnp.where(band, 0.0, NEG)
    lead[...] = place[:, :HEAD_DIM]

    def relay(h):
        for k in PEERS:
            with scope(f"relay_{h}_{k}"):
                x_kv(h, k).wait_recv()
            y_send([(h, k)])

    def near(h):
        cols = slice(h * HEAD_DIM, (h + 1) * HEAD_DIM)
        for b in range(2):
            span = slice(b * 2 * SIDE, (b + 1) * 2 * SIDE)
            keys = slice(b * 2 * SIDE, b * 2 * SIDE + 4 * SIDE)
            m, l, acc = attend(qn[span, cols], kn[keys, cols], vn[keys, cols], near_bias[b])
            nm[h, span] = m
            nl[h, span] = l
            nacc[h, span] = acc

    def give_back(h, k):
        s = xpeer(k)
        return [
            remote(sret.at[h, s], ret.at[h, x], rs.at[0], rr.at[h, 0], (base + s, tp)),
            remote(sstat.at[h, s], rstat.at[h, x], rs.at[1], rr.at[h, 1], (base + s, tp)),
        ]

    def residue_wait(h):
        with scope(f"wait_q_{h}"):
            taken(qres.at[h, pl.ds(0, ROW - 1)], qr.at[h])
        with scope(f"wait_y_{h}"):
            y_wait(h)

    def residue_work(h):
        far, mid = [], []
        for d in range(SUB):
            q = qres[h, :, d].reshape(SIDE, HEAD_DIM)
            k = kvres[h, :, 0, d].reshape(3 * SIDE, HEAD_DIM)
            v = kvres[h, :, 1, d].reshape(3 * SIDE, HEAD_DIM)
            q = jnp.concatenate([q, q], axis=0)
            k = jnp.concatenate([k, k[:SIDE]], axis=0)
            v = jnp.concatenate([v, v[:SIDE]], axis=0)
            far.append([a[:SIDE] for a in attend(q, k, v, far_bias[...])])
        for e in range(2):
            two = slice(2 * e, 2 * e + 2)
            q = qres[h, two].reshape(2 * SIDE, HEAD_DIM)
            k = kvres[h, 2 * e + 3 : 2 * e + 7, 0].reshape(4 * SIDE, HEAD_DIM)
            v = kvres[h, 2 * e + 3 : 2 * e + 7, 1].reshape(4 * SIDE, HEAD_DIM)
            mid.append(attend(q, k, v, mid_bias[e]))
        lses = []
        for s in range(ROW):
            part = slice(s % 2 * SIDE, (s % 2 + 1) * SIDE)
            m1, l1, acc1 = (mid[s // 2][i][part] for i in range(3))
            part = slice(s * BLK, (s + 1) * BLK)
            m2, l2, acc2 = (
                jnp.concatenate([f[i][part] for f in far], axis=0) for i in range(3)
            )
            m = jnp.maximum(m1, m2)
            a1, a2 = jnp.exp2(m1 - m), jnp.exp2(m2 - m)
            l = a1 * l1 + a2 * l2
            sret[h, s] = ((a1 * acc1 + a2 * acc2) / l).astype(BF)
            lses.append(m + jnp.log2(l))
        for e in range(2):
            flat = jnp.transpose(jnp.concatenate(lses[2 * e : 2 * e + 2], axis=0))
            sstat[h, 2 * e] = flat[:1]
            sstat[h, 2 * e + 1] = flat[:1]

    def residue(*which):
        for h in which:
            residue_wait(h)
        for h in which:
            residue_work(h)
        for h in which:
            for k in SENDS:
                for copy in give_back(h, k):
                    copy.start()
        for h in which:
            ret[h, x] = sret[h, x]
            rstat[h, x] = sstat[h, x]

    def columns(h, side):
        return pl.ds(pl.multiple_of((side * heads + h) * HEAD_DIM, HEAD_DIM), HEAD_DIM)

    def tp_copy(h):
        mine = out_ref.at[:, columns(h, tp)]
        return remote(mine, mine, ts.at[0], ts.at[1], (sp, 1 - tp))

    def combine(h):
        with scope(f"wait_back_{h}"):
            taken(ret.at[h, pl.ds(0, ROW - 1)], rr.at[h, 0])
            taken(rstat.at[h, pl.ds(0, ROW - 1)], rr.at[h, 1])
        got = ret[h].reshape(rows, HEAD_DIM)
        out = jnp.dot(unperm, got, preferred_element_type=F32)
        lane = iota((rows, HEAD_DIM), 1)
        small = iota((1, HEAD_DIM), 1)
        odd = jnp.broadcast_to(x & 1, (1, HEAD_DIM)) == 1
        where = lead[...]
        col = jnp.zeros((rows, HEAD_DIM), F32)
        for pair in range(2):
            one, two = rstat[h, 2 * pair], rstat[h, 2 * pair + 1]
            one = jnp.where(odd, pltpu.roll(one, SIDE, 1), one)
            two = jnp.where(odd, two, pltpu.roll(two, SIDE, 1))
            row = jnp.where(small < piece, one, two)
            col = jnp.where(where == lane + pair * HEAD_DIM, row, col)
        lse = jnp.broadcast_to(jnp.sum(col, axis=1, keepdims=True), col.shape)
        m0 = nm[h]
        m = jnp.maximum(m0, lse)
        a0, a1 = jnp.exp2(m0 - m), jnp.exp2(lse - m)
        att = (a0 * nacc[h] + a1 * out) / (a0 * nl[h] + a1)
        out_ref[:, columns(h, tp)] = att.astype(BF)
        tp_copy(h).start()

    relay(0)
    relay(1)
    relay(2)
    relay(3)
    halo_send((to_right & (x == ROW - 1), to_left & (x == 0)))
    for h in range(heads):
        residue(h)
    with scope("wait_halo"):
        halo_wait(nr, halo_in)
    for h in range(heads):
        near(h)
    for h in range(heads):
        combine(h)

    with scope("send_waits"):
        taken(xkv.at[pl.ds(0, ROW - 1)], xs.at[0])
        taken(xq.at[pl.ds(0, ROW - 1)], xs.at[1])
        for way, side in enumerate(y_out):
            @pl.when(side)
            def _():
                taken(xkv, ys.at[way])
        halo_wait(ns, halo_out)
        taken(sret.at[:, pl.ds(0, ROW - 1)], rs.at[0])
        taken(sstat.at[:, pl.ds(0, ROW - 1)], rs.at[1])
    with scope("wait_tp"):
        taken(qn, ts.at[1])
        taken(qn, ts.at[0])


def per_device(n, queries, keys, values, w_out):
    rows, columns = queries.shape
    heads = columns // HEAD_DIM
    vmem = pltpu.VMEM
    dma = pltpu.SemaphoreType.DMA
    attended = pl.pallas_call(
        functools.partial(kernel, n, heads),
        out_shape=jax.ShapeDtypeStruct((rows, 2 * columns), BF),
        in_specs=[pl.BlockSpec(memory_space=pltpu.HBM)] * 3,
        out_specs=pl.BlockSpec(memory_space=pltpu.VMEM),
        scratch_shapes=[
            vmem((rows, columns), BF),
            vmem((rows + 2 * SIDE, columns), BF),
            vmem((rows + 2 * SIDE, columns), BF),
            vmem((ROW, heads, 2, SUB, BLK, HEAD_DIM), BF),
            vmem((ROW, heads, SUB, BLK, HEAD_DIM), BF),
            vmem((heads, 3 * ROW, 2, SUB, BLK, HEAD_DIM), BF),
            vmem((heads, ROW, SUB, BLK, HEAD_DIM), BF),
            vmem((heads, ROW, SIDE, HEAD_DIM), BF),
            vmem((heads, ROW, 1, HEAD_DIM), F32),
            vmem((heads, ROW, SIDE, HEAD_DIM), BF),
            vmem((heads, ROW, 1, HEAD_DIM), F32),
            vmem((heads, rows, HEAD_DIM), F32),
            vmem((heads, rows, HEAD_DIM), F32),
            vmem((heads, rows, HEAD_DIM), F32),
            vmem((2, 2 * SIDE, 4 * SIDE), F32),
            vmem((2, 2 * SIDE, 4 * SIDE), F32),
            vmem((2 * SIDE, 4 * SIDE), F32),
            vmem((rows, HEAD_DIM), jnp.int32),
            dma((3,)),
            dma((2,)),
            dma((heads, ROW - 1)),
            dma((heads,)),
            dma((2,)),
            dma((heads, 2)),
            dma((2,)),
            dma((2,)),
            dma((2,)),
            dma((heads, 2)),
            dma((2,)),
        ],
        compiler_params=pltpu.CompilerParams(
            collective_id=0, has_side_effects=True, vmem_limit_bytes=20 * 1024 * 1024
        ),
        name="fused",
    )(*(pltpu.with_memory_space_constraint(a, pltpu.HBM) for a in (queries, keys, values)))
    return jnp.dot(attended, w_out, preferred_element_type=F32).astype(BF)


def solution(mesh):
    return jax.shard_map(
        functools.partial(per_device, mesh.shape["sp"]),
        mesh=mesh,
        in_specs=(P("sp", "tp"), P("sp", "tp"), P("sp", "tp"), P(None, "tp")),
        out_specs=P("sp", "tp"),
        check_vma=False,
    )
```

```python
import functools
import math

import jax
import jax.numpy as jnp
from jax import lax
from jax.experimental import pallas as pl
from jax.experimental.pallas import tpu as pltpu
from jax.sharding import PartitionSpec as P

HEAD_DIM = 128
SIDE = 64
ROW = 4
SUB = 4
BLK = 16
MESH = pl.DeviceIdType.MESH
scope = jax.named_scope
BF, F32 = jnp.bfloat16, jnp.float32
NEG = -1e30
COEF = math.log2(math.e) / math.sqrt(HEAD_DIM)
PEERS = (1, 3, 2)
SENDS = (1, 3, 2)


def attend(q, k, v, bias):
    s = lax.dot_general(q, k, (((1,), (1,)), ((), ())), preferred_element_type=F32)
    t = s * COEF + bias
    m = jnp.max(t, axis=1, keepdims=True)
    p = jnp.exp2(t - m)
    l = jnp.sum(p, axis=1, keepdims=True)
    acc = jnp.dot(p.astype(BF), v, preferred_element_type=F32)
    return jnp.broadcast_to(m, acc.shape), jnp.broadcast_to(l, acc.shape), acc


def kernel(
    n, heads, q_hbm, k_hbm, v_hbm, out_ref,
    qn, kn, vn, xkv, xq, kvres, qres, sret, sstat, ret, rstat,
    nacc, nm, nl, near_bias, mid_bias, far_bias, lead,
    lsem, xs, xr, qr, ys, yr, ns, nr, rs, rr, ts,
):
    sp, tp = lax.axis_index("sp"), lax.axis_index("tp")
    x = lax.rem(sp, ROW)
    base = sp - x
    up = lax.rem(sp + ROW, n)
    down = lax.rem(sp + n - ROW, n)
    right = lax.rem(sp + 1, n)
    left = lax.rem(sp + n - 1, n)
    rows = qn.shape[0]
    piece = rows // ROW

    loads = [
        pltpu.make_async_copy(k_hbm, kn.at[pl.ds(SIDE, rows)], lsem.at[0]),
        pltpu.make_async_copy(v_hbm, vn.at[pl.ds(SIDE, rows)], lsem.at[1]),
        pltpu.make_async_copy(q_hbm, qn, lsem.at[2]),
    ]
    for copy in loads:
        copy.start()

    def xpeer(k):
        return lax.rem(x + k, ROW)

    first = (sp < ROW).astype(jnp.int32)
    last = (sp >= n - ROW).astype(jnp.int32)
    start = (sp == 0).astype(jnp.int32)
    end = (sp == n - 1).astype(jnp.int32)
    to_up, to_down, to_right, to_left = sp < n - ROW, sp >= ROW, sp < n - 1, sp >= 1

    barrier = pltpu.get_barrier_semaphore()

    def greet(friend):
        pl.semaphore_signal(barrier, inc=1, device_id=friend, device_id_type=MESH)

    for k in PEERS:
        greet((base + xpeer(k), tp))
    greet((sp, 1 - tp))
    pl.when(to_up)(lambda: greet((up, tp)))
    pl.when(to_down)(lambda: greet((down, tp)))
    pl.when(to_right)(lambda: greet((right, tp)))
    pl.when(to_left)(lambda: greet((left, tp)))

    def iota(shape, dim):
        return lax.broadcasted_iota(jnp.int32, shape, dim)

    r, t = iota((rows, rows), 0), iota((rows, rows), 1)
    order = (r & 15) * 16 + ((r >> 4) & 3) * 4 + (r >> 6)
    perm = jnp.where(t == order, 1.0, 0.0).astype(BF)
    place = (r & 3) * 64 + ((r >> 2) & 3) * 16 + (r >> 4)
    unperm = jnp.where(t == place, 1.0, 0.0).astype(BF)

    with scope("load_k"):
        loads[0].wait()
    kp = jnp.dot(perm, kn[SIDE : SIDE + rows], preferred_element_type=F32).astype(BF)
    with scope("load_v"):
        loads[1].wait()
    vp = jnp.dot(perm, vn[SIDE : SIDE + rows], preferred_element_type=F32).astype(BF)

    def cut(a, c, h):
        a = a[c * piece : (c + 1) * piece, h * HEAD_DIM : (h + 1) * HEAD_DIM]
        return a.reshape(SUB, BLK, HEAD_DIM)

    for h in range(heads):
        for c in range(ROW):
            xkv[c, h, 0] = cut(kp, c, h)
            xkv[c, h, 1] = cut(vp, c, h)

    with scope("barrier"):
        pl.semaphore_wait(barrier, 2 * ROW - first - last - start - end)

    def remote(src, dst, ssem, rsem, device):
        return pltpu.make_async_remote_copy(
            src_ref=src, dst_ref=dst, send_sem=ssem, recv_sem=rsem,
            device_id=device, device_id_type=MESH,
        )

    def x_kv(h, k):
        c = xpeer(k)
        return remote(
            xkv.at[c, h], kvres.at[h, ROW + x], xs.at[0], xr.at[h, k - 1], (base + c, tp)
        )

    def x_q(h, k):
        c = xpeer(k)
        return remote(xq.at[c, h], qres.at[h, x], xs.at[1], qr.at[h], (base + c, tp))

    def y_kv(h, k, way):
        s = xpeer(ROW - k)
        region = 0 if way == 0 else 2 * ROW
        return remote(
            xkv.at[x, h] if k == 0 else kvres.at[h, ROW + s], kvres.at[h, region + s],
            ys.at[way], yr.at[h, way], (up if way == 0 else down, tp),
        )

    def taken(ref, sem):
        remote(ref, ref, sem, sem, (sp, 1 - tp)).wait_recv()

    def y_send(pairs):
        for way, side in enumerate(y_out):
            @pl.when(side)
            def _():
                for h, k in pairs:
                    y_kv(h, k, way).start()

    def y_wait(h):
        for way, side in enumerate(y_in):
            @pl.when(side)
            def _():
                taken(kvres.at[h, pl.ds(0, ROW)], yr.at[h, way])

    def halo_send(sides):
        for way, side in enumerate(sides):
            @pl.when(side)
            def _():
                for a in (kn, vn):
                    if way == 0:
                        src, dst, who = pl.ds(rows, SIDE), pl.ds(0, SIDE), right
                    else:
                        src, dst, who = pl.ds(SIDE, SIDE), pl.ds(SIDE + rows, SIDE), left
                    remote(a.at[src], a.at[dst], ns.at[way], nr.at[way], (who, tp)).start()

    def halo_wait(sems, sides):
        for way, side in enumerate(sides):
            @pl.when(side)
            def _():
                taken(kn.at[pl.ds(0, 2 * SIDE)], sems.at[way])

    y_out, y_in = (to_up, to_down), (to_down, to_up)
    halo_out, halo_in = (to_right, to_left), (to_left, to_right)

    def first_sends():
        for h in range(heads - 1):
            for k in SENDS:
                x_kv(h, k).start()
        y_send([(h, 0) for h in range(heads)])

    def second_sends():
        for h in range(heads):
            for k in SENDS:
                x_q(h, k).start()
            if h == 0:
                for k in SENDS:
                    x_kv(heads - 1, k).start()
        halo_send((to_right & (x < ROW - 1), to_left & (x > 0)))

    pl.when(tp == 0)(first_sends)
    with scope("load_q"):
        loads[2].wait()
    qp = jnp.dot(perm, qn[...], preferred_element_type=F32).astype(BF)
    for h in range(heads):
        for c in range(ROW):
            xq[c, h] = cut(qp, c, h)
    pl.when(tp == 0)(second_sends)
    for h in range(heads):
        kvres[h, ROW + x] = xkv[x, h]
        qres[h, x] = xq[x, h]

    blank = jnp.zeros((heads, ROW, 2, SUB, BLK, HEAD_DIM), BF)
    edge = jnp.zeros((SIDE, heads * HEAD_DIM), BF)

    @pl.when(sp < ROW)
    def _():
        kvres[:, :ROW] = blank

    @pl.when(sp >= n - ROW)
    def _():
        kvres[:, 2 * ROW :] = blank

    @pl.when(sp == 0)
    def _():
        kn[:SIDE] = edge
        vn[:SIDE] = edge

    @pl.when(sp == n - 1)
    def _():
        kn[SIDE + rows :] = edge
        vn[SIDE + rows :] = edge

    iq, ik = iota((2 * SIDE, 4 * SIDE), 0), iota((2 * SIDE, 4 * SIDE), 1)
    band = (ik >= iq) & (ik <= iq + 2 * SIDE)
    near_bias[0] = jnp.where(band & (ik >= start * SIDE), 0.0, NEG)
    near_bias[1] = jnp.where(band & (ik < 4 * SIDE - end * SIDE), 0.0, NEG)
    low, high = first * SIDE, (4 - last) * SIDE
    wq = (iq >> 6) * 64 + (iq & 15) * 4 + ((iq >> 4) & 3)
    wk = (ik >> 6) * 64 - SIDE + (ik & 15) * 4 + ((ik >> 4) & 3)
    band = (wk - wq <= SIDE) & (wq - wk <= SIDE)
    mid_bias[0] = jnp.where(band & (ik >= low), 0.0, NEG)
    mid_bias[1] = jnp.where(band & (ik < high), 0.0, NEG)
    iq = iq & (SIDE - 1)
    band = (ik >= iq) & (ik <= iq + 2 * SIDE)
    band = band & (ik >= first * SIDE) & (ik < (3 - last) * SIDE)
    far_bias[...] = jnp.where(band, 0.0, NEG)
    lead[...] = place[:, :HEAD_DIM]

    @pl.when(tp == 1)
    def _():
        first_sends()
        second_sends()

    def relay(h):
        for k in PEERS:
            with scope(f"relay_{h}_{k}"):
                x_kv(h, k).wait_recv()
            y_send([(h, k)])

    def near(h, b):
        cols = slice(h * HEAD_DIM, (h + 1) * HEAD_DIM)
        span = slice(b * 2 * SIDE, (b + 1) * 2 * SIDE)
        keys = slice(b * 2 * SIDE, b * 2 * SIDE + 4 * SIDE)
        m, l, acc = attend(qn[span, cols], kn[keys, cols], vn[keys, cols], near_bias[b])
        nm[h, span] = m
        nl[h, span] = l
        nacc[h, span] = acc

    def give_back(h, k):
        s = xpeer(k)
        return [
            remote(sret.at[h, s], ret.at[h, x], rs.at[0], rr.at[h, 0], (base + s, tp)),
            remote(sstat.at[h, s], rstat.at[h, x], rs.at[1], rr.at[h, 1], (base + s, tp)),
        ]

    def residue_wait(h):
        with scope(f"wait_q_{h}"):
            taken(qres.at[h, pl.ds(0, ROW - 1)], qr.at[h])
        with scope(f"wait_y_{h}"):
            y_wait(h)

    def residue_work(h):
        far, mid = [], []
        for d in range(SUB):
            q = qres[h, :, d].reshape(SIDE, HEAD_DIM)
            k = kvres[h, :, 0, d].reshape(3 * SIDE, HEAD_DIM)
            v = kvres[h, :, 1, d].reshape(3 * SIDE, HEAD_DIM)
            q = jnp.concatenate([q, q], axis=0)
            k = jnp.concatenate([k, k[:SIDE]], axis=0)
            v = jnp.concatenate([v, v[:SIDE]], axis=0)
            far.append([a[:SIDE] for a in attend(q, k, v, far_bias[...])])
        for e in range(2):
            two = slice(2 * e, 2 * e + 2)
            q = qres[h, two].reshape(2 * SIDE, HEAD_DIM)
            k = kvres[h, 2 * e + 3 : 2 * e + 7, 0].reshape(4 * SIDE, HEAD_DIM)
            v = kvres[h, 2 * e + 3 : 2 * e + 7, 1].reshape(4 * SIDE, HEAD_DIM)
            mid.append(attend(q, k, v, mid_bias[e]))
        lses = []
        for s in range(ROW):
            part = slice(s % 2 * SIDE, (s % 2 + 1) * SIDE)
            m1, l1, acc1 = (mid[s // 2][i][part] for i in range(3))
            part = slice(s * BLK, (s + 1) * BLK)
            m2, l2, acc2 = (
                jnp.concatenate([f[i][part] for f in far], axis=0) for i in range(3)
            )
            m = jnp.maximum(m1, m2)
            a1, a2 = jnp.exp2(m1 - m), jnp.exp2(m2 - m)
            l = a1 * l1 + a2 * l2
            sret[h, s] = ((a1 * acc1 + a2 * acc2) / l).astype(BF)
            lses.append(m + jnp.log2(l))
        for e in range(2):
            flat = jnp.transpose(jnp.concatenate(lses[2 * e : 2 * e + 2], axis=0))
            sstat[h, 2 * e] = flat[:1]
            sstat[h, 2 * e + 1] = flat[:1]

    def residue(*which):
        for h in which:
            residue_wait(h)
        for h in which:
            residue_work(h)
        for h in which:
            for k in SENDS:
                for copy in give_back(h, k):
                    copy.start()
        for h in which:
            ret[h, x] = sret[h, x]
            rstat[h, x] = sstat[h, x]

    def columns(h, side):
        return pl.ds(pl.multiple_of((side * heads + h) * HEAD_DIM, HEAD_DIM), HEAD_DIM)

    def tp_copy(h):
        mine = out_ref.at[:, columns(h, tp)]
        return remote(mine, mine, ts.at[0], ts.at[1], (sp, 1 - tp))

    def combine(h):
        with scope(f"wait_back_{h}"):
            taken(ret.at[h, pl.ds(0, ROW - 1)], rr.at[h, 0])
            taken(rstat.at[h, pl.ds(0, ROW - 1)], rr.at[h, 1])
        got = ret[h].reshape(rows, HEAD_DIM)
        out = jnp.dot(unperm, got, preferred_element_type=F32)
        lane = iota((rows, HEAD_DIM), 1)
        small = iota((1, HEAD_DIM), 1)
        odd = jnp.broadcast_to(x & 1, (1, HEAD_DIM)) == 1
        where = lead[...]
        col = jnp.zeros((rows, HEAD_DIM), F32)
        for pair in range(2):
            one, two = rstat[h, 2 * pair], rstat[h, 2 * pair + 1]
            one = jnp.where(odd, pltpu.roll(one, SIDE, 1), one)
            two = jnp.where(odd, two, pltpu.roll(two, SIDE, 1))
            row = jnp.where(small < piece, one, two)
            col = jnp.where(where == lane + pair * HEAD_DIM, row, col)
        lse = jnp.broadcast_to(jnp.sum(col, axis=1, keepdims=True), col.shape)
        m0 = nm[h]
        m = jnp.maximum(m0, lse)
        a0, a1 = jnp.exp2(m0 - m), jnp.exp2(lse - m)
        att = (a0 * nacc[h] + a1 * out) / (a0 * nl[h] + a1)
        out_ref[:, columns(h, tp)] = att.astype(BF)
        tp_copy(h).start()

    relay(0)
    relay(1)
    relay(2)
    relay(3)
    halo_send((to_right & (x == ROW - 1), to_left & (x == 0)))
    for h in range(heads):
        residue(h)
    for b in (1, 0):
        with scope(f"wait_halo_{b}"):
            halo_wait(nr, tuple(side if way == b else sp < 0 for way, side in enumerate(halo_in)))
        for h in range(heads):
            near(h, b)
    for h in range(heads):
        combine(h)

    with scope("send_waits"):
        taken(xkv.at[pl.ds(0, ROW - 1)], xs.at[0])
        taken(xq.at[pl.ds(0, ROW - 1)], xs.at[1])
        for way, side in enumerate(y_out):
            @pl.when(side)
            def _():
                taken(xkv, ys.at[way])
        halo_wait(ns, halo_out)
        taken(sret.at[:, pl.ds(0, ROW - 1)], rs.at[0])
        taken(sstat.at[:, pl.ds(0, ROW - 1)], rs.at[1])
    with scope("wait_tp"):
        taken(qn, ts.at[1])
        taken(qn, ts.at[0])


def per_device(n, queries, keys, values, w_out):
    rows, columns = queries.shape
    heads = columns // HEAD_DIM
    vmem = pltpu.VMEM
    dma = pltpu.SemaphoreType.DMA
    attended = pl.pallas_call(
        functools.partial(kernel, n, heads),
        out_shape=jax.ShapeDtypeStruct((rows, 2 * columns), BF),
        in_specs=[pl.BlockSpec(memory_space=pltpu.HBM)] * 3,
        out_specs=pl.BlockSpec(memory_space=pltpu.VMEM),
        scratch_shapes=[
            vmem((rows, columns), BF),
            vmem((rows + 2 * SIDE, columns), BF),
            vmem((rows + 2 * SIDE, columns), BF),
            vmem((ROW, heads, 2, SUB, BLK, HEAD_DIM), BF),
            vmem((ROW, heads, SUB, BLK, HEAD_DIM), BF),
            vmem((heads, 3 * ROW, 2, SUB, BLK, HEAD_DIM), BF),
            vmem((heads, ROW, SUB, BLK, HEAD_DIM), BF),
            vmem((heads, ROW, SIDE, HEAD_DIM), BF),
            vmem((heads, ROW, 1, HEAD_DIM), F32),
            vmem((heads, ROW, SIDE, HEAD_DIM), BF),
            vmem((heads, ROW, 1, HEAD_DIM), F32),
            vmem((heads, rows, HEAD_DIM), F32),
            vmem((heads, rows, HEAD_DIM), F32),
            vmem((heads, rows, HEAD_DIM), F32),
            vmem((2, 2 * SIDE, 4 * SIDE), F32),
            vmem((2, 2 * SIDE, 4 * SIDE), F32),
            vmem((2 * SIDE, 4 * SIDE), F32),
            vmem((rows, HEAD_DIM), jnp.int32),
            dma((3,)),
            dma((2,)),
            dma((heads, ROW - 1)),
            dma((heads,)),
            dma((2,)),
            dma((heads, 2)),
            dma((2,)),
            dma((2,)),
            dma((2,)),
            dma((heads, 2)),
            dma((2,)),
        ],
        compiler_params=pltpu.CompilerParams(
            collective_id=0, has_side_effects=True, vmem_limit_bytes=20 * 1024 * 1024
        ),
        name="fused",
    )(*(pltpu.with_memory_space_constraint(a, pltpu.HBM) for a in (queries, keys, values)))
    return jnp.dot(attended, w_out, preferred_element_type=F32).astype(BF)


def solution(mesh):
    return jax.shard_map(
        functools.partial(per_device, mesh.shape["sp"]),
        mesh=mesh,
        in_specs=(P("sp", "tp"), P("sp", "tp"), P("sp", "tp"), P(None, "tp")),
        out_specs=P("sp", "tp"),
        check_vma=False,
    )
```
